256 devices in a mesh: st: 64 (over z, y, core), tp: 4 (over x).
Axes of the slice: x: 4, y: 4, z: 8, core: 2. Of those that a mesh axis runs over, the one named last changes fastest.
Arguments:
- queries: bfloat16 [65536, 1024], P('st', 'tp'), may hold values from -540 to 540
- gate_pre: bfloat16 [65536, 1024], P('st', 'tp'), may hold values from -6 to 6
- cotangent: bfloat16 [65536, 1024], P('st', 'tp'), may hold values from -6 to 6
- store: bfloat16 [81920, 2048], P('st'), may hold values from -6 to 6
- store_gain: float32 [2048], replicated, may hold values from 0.1 to 1.9
- w_key: bfloat16 [2048, 1024], P(None, 'tp'), may hold values from -0.125 to 0.125
- w_value: bfloat16 [2048, 1024], P(None, 'tp'), may hold values from -0.125 to 0.125
- owners: int32 [512, 4], P('st'), may hold values from 0 to 63, all different within a row; in each aligned block of 8 rows (0 to 7, 8 to 15, ...) at most 1 rows name the same one
- slots: int32 [512, 4], P('st'), may hold values from 0 to 19
Outputs:
- grad_queries: float32 [65536, 1024], P('st', 'tp')
- grad_store: float32 [81920, 2048], P(('st', 'tp'))
- grad_w_value: float32 [2048, 1024], P('st', 'tp')
The draws below stay inside these ranges and needn't reach their ends.
Inputs may be any that keep to these rules, and one draw needn't show every extreme that they name: Each block names 4 different owners. Among the blocks of one device no owner is named twice.
All inputs are finite; a program needn't handle non-finite values.
Results may differ from the reference program's by a relative error of at most 0.014.
Values may be sent and summed in bfloat16 or wider, within the bound.
A program may use at most 192 MiB of HBM per device.

```python
import math
import jax
import jax.numpy as jnp
import numpy as np
from jax import lax

D = 2048
HEADS = 8
HD = 128
PLEN = 64
BLK = 128
NPB = 4
PASS_DEV = 20
XW = 1024
BLK_DEV = 8
CAP = 1
TOKENS = 65536
BLOCKS = 512
PASSAGES = 1280
ROWS = 81920
N_ST = 64


def draw_queries(key, part):
    first_key = jax.random.fold_in(key, 11)
    drawn = jnp.clip(jax.random.normal(first_key, (TOKENS, XW), jnp.float32), -6.0, 6.0)
    return drawn.astype(jnp.bfloat16)


def draw_cotangent(key, part):
    first_key = jax.random.fold_in(key, 13)
    drawn = jnp.clip(jax.random.normal(first_key, (TOKENS, XW), jnp.float32), -6.0, 6.0)
    return drawn.astype(jnp.bfloat16)


def set_ends(array, stream_key, least, high):
    place = [jax.random.randint(jax.random.fold_in(stream_key, axis), (), 0, length) for axis, length in enumerate(array.shape)]
    widest = array.shape.index(max(array.shape))
    neighbour = place[:widest] + [(place[widest] + 1) % array.shape[widest]] + place[widest + 1:]
    return array.at[tuple(place)].set(least).at[tuple(neighbour)].set(high)


def shard_levels(key, extent, shards, low, largest):
    gain = 1.0
    for position, shards_of in shards:
        heights = jax.random.uniform(jax.random.fold_in(jax.random.fold_in(key, 6), position), (shards_of,), jnp.float32, low / len(shards), largest / len(shards))
        gain = gain * jnp.repeat(jnp.exp(heights), extent[position] // shards_of).reshape((-1,) + (1,) * (len(extent) - 1 - position))
    return gain


def rank_bounds(number_of, skew):
    portions = [(1 << 20) // math.isqrt(grade ** skew) + 1 for grade in range(1, number_of + 1)]
    width = 1 + sum(portions) // (1 << 30)
    return np.cumsum(np.array([max(1, weight // width) for weight in portions]))


def ranked_ids(rng, dims, count, skew):
    table = rank_bounds(count, skew)
    lot = jax.random.randint(jax.random.fold_in(rng, 1), dims, 0, int(table[count - 1]))
    standing = jnp.searchsorted(jnp.asarray(table, jnp.int32), lot, side="right")
    return jax.random.permutation(jax.random.fold_in(rng, 2), count)[standing].astype(jnp.int32)


def routed_block(own_key, own, number, rows, count, top, bound, lean):
    sequence = jax.random.permutation(own_key, count)
    heavy_load, common = portions_of(count, rows * top, bound, lean, True), portions_of(count, rows * top, bound, lean, False)
    places = jnp.arange(count)

    def named(lengths, rotation):
        used = int((lengths > 0).sum())
        fixed = max(1, used // 4)
        moved = fixed + (places - fixed + rotation * (used - fixed)) % max(1, count - fixed)
        return jnp.zeros((count,), jnp.int32).at[sequence[jnp.where(places < fixed, places, moved)]].set(jnp.asarray(lengths, jnp.int32))

    lengths = jnp.where(number % 4 == 0, named(heavy_load, number // 4), named(common, number - number // 4 - 1))
    mixed = jax.random.permutation(jax.random.fold_in(own, 3), count)
    giver, sink = mixed[0:count // 2 * 2:2], mixed[1:count // 2 * 2:2]
    room = jnp.minimum(lengths[giver] - 1, bound - lengths[sink]) // 2
    room = jnp.where((giver == sequence[0]) | (sink == sequence[0]) | (lengths[sink] == 0), 0, jnp.maximum(room, 0))
    moved = jax.random.randint(jax.random.fold_in(own, 4), (count // 2,), 0, 1 << 20) % (room + 1)
    lengths = lengths.at[giver].add(-moved).at[sink].add(moved)
    labels = jnp.searchsorted(jnp.cumsum(lengths), jnp.arange(rows * top), side="right").astype(jnp.int32)
    listing = labels.reshape(top, rows).T
    listing = listing[jax.random.permutation(jax.random.fold_in(own, 1), rows)]
    rotation = jax.random.randint(jax.random.fold_in(own, 2), (rows, 1), 0, top)
    return jnp.take_along_axis(listing, (jnp.arange(top)[None, :] + rotation) % top, axis=1)


def portions_of(amount, total, bound, slope, full):
    weights = [(1 << 20) // math.isqrt(rank ** slope) + 1 for rank in range(1, amount + 1)]
    largest = bound if full else min(bound, max(-(-total // amount), total * weights[0] // sum(weights)))
    least = 1 if total - largest >= amount - 1 else 0
    counts, surplus = [largest] + [least] * (amount - 1), total - largest - least * (amount - 1)
    while surplus > 0:
        movable = [i for i in range(1, amount) if counts[i] < largest] or [i for i in range(1, amount) if counts[i] < bound]
        whole, budget = sum([weights[i] for i in movable]), surplus
        for i in movable:
            addition = min(bound - counts[i], max(1, budget * weights[i] // whole), surplus)
            counts[i] = counts[i] + addition
            surplus = surplus - addition
    return np.array(counts)


def normal_values(own_key, dims, scale, bound, split=(), kind=jnp.bfloat16):
    factor_of = shard_levels(own_key, dims, split, -0.22, 0.18) if split else 1.0
    values = jax.random.normal(own_key, dims, jnp.float32) * scale * factor_of
    return jnp.minimum(jnp.maximum(values, -bound), bound).astype(kind)


def setup_inputs(seed: int = 0) -> dict:
    key_of = jax.random.split(jax.random.key(seed), 10)
    queries = draw_queries(jax.random.fold_in(key_of[9], 71), 0)
    gate_pre = normal_values(key_of[1], (TOKENS, XW), 1.5, 6.0, ((0, 64), (1, 4)))
    cotangent = draw_cotangent(jax.random.fold_in(key_of[9], 71), 0)
    store = normal_values(key_of[3], (ROWS, D), 1.0, 6.0, ((0, 64),))
    store_gain = jnp.clip(1.0 + 0.18 * jax.random.normal(key_of[4], (D,), jnp.float32), 0.1, 1.9)
    w_key = normal_values(key_of[5], (D, XW), D ** -0.5, 0.125, ((1, 4),))
    w_value = normal_values(key_of[6], (D, XW), D ** -0.5, 0.125, ((1, 4),))
    owners_keys = jax.random.split(jax.random.fold_in(key_of[7], 1), BLOCKS // BLK_DEV)
    owners_turns = jax.random.permutation(jax.random.fold_in(key_of[7], 3), BLOCKS // BLK_DEV)
    owners = jax.vmap(lambda own, number: routed_block(jax.random.fold_in(key_of[7], 2), own, number, BLK_DEV, N_ST, NPB, CAP, 2))(owners_keys, owners_turns).reshape((BLOCKS, NPB))
    slots = set_ends(ranked_ids(key_of[8], (BLOCKS, NPB), PASS_DEV, 2), jax.random.fold_in(key_of[8], 3), 0, PASS_DEV - 1).astype(jnp.int32)
    return {"queries": queries, "gate_pre": gate_pre, "cotangent": cotangent, "store": store, "store_gain": store_gain, "w_key": w_key, "w_value": w_value, "owners": owners, "slots": slots}


EPS = 1e-06

def reference(queries, gate_pre, cotangent, store, store_gain, w_key, w_value, owners, slots):
    store_rows = store.astype(jnp.float32)
    row_inverse = lax.rsqrt(lax.optimization_barrier(jnp.mean(store_rows * store_rows, axis=-1, keepdims=True)) + EPS)
    normed = (store_rows * row_inverse * store_gain).astype(jnp.bfloat16)
    key_table = jnp.dot(normed, w_key, preferred_element_type=jnp.float32).astype(jnp.bfloat16).reshape(PASSAGES, PLEN, XW)
    value_table = jnp.dot(normed, w_value, preferred_element_type=jnp.float32).astype(jnp.bfloat16).reshape(PASSAGES, PLEN, XW)
    passage_ids = (owners * PASS_DEV + slots).astype(jnp.int32)
    score_scale = HD ** (-0.5)

    def one_group(group):
        query_part, gate_part, cot_part, id_part = group
        flat_ids = id_part.reshape(-1).astype(jnp.int32)
        group_keys = key_table[flat_ids].reshape(BLK_DEV, NPB * PLEN, HEADS, HD).astype(jnp.float32)
        group_values = value_table[flat_ids].reshape(BLK_DEV, NPB * PLEN, HEADS, HD).astype(jnp.float32)
        query_wide = query_part.astype(jnp.float32)
        scores = jnp.einsum('bqhd,bkhd->bhqk', query_wide, group_keys) * score_scale
        shifted = scores - lax.optimization_barrier(jnp.max(scores, axis=-1, keepdims=True))
        weights = jnp.exp(shifted)
        weights = weights / lax.optimization_barrier(jnp.sum(weights, axis=-1, keepdims=True))
        weights_half = lax.optimization_barrier(weights.astype(jnp.bfloat16)).astype(jnp.float32)
        grad_in = jax.nn.sigmoid(gate_part.astype(jnp.float32)) * cot_part.astype(jnp.float32)
        grad_in = lax.optimization_barrier(grad_in.astype(jnp.bfloat16)).astype(jnp.float32)
        attended = jnp.einsum('bhqk,bkhd->bqhd', weights_half, group_values)
        row_delta = lax.optimization_barrier(jnp.sum(grad_in * attended, axis=-1))
        grad_weights = jnp.einsum('bqhd,bkhd->bhqk', grad_in, group_values)
        grad_scores = weights * (grad_weights - jnp.transpose(row_delta, (0, 2, 1))[..., None])
        grad_half = lax.optimization_barrier(grad_scores.astype(jnp.bfloat16)).astype(jnp.float32)
        grad_query = jnp.einsum('bhqk,bkhd->bqhd', grad_half, group_keys) * score_scale
        grad_key = jnp.einsum('bhqk,bqhd->bkhd', grad_half, query_wide) * score_scale
        grad_value = jnp.einsum('bhqk,bqhd->bkhd', weights_half, grad_in)
        return (grad_query.reshape(BLK_DEV * BLK, XW), grad_key.reshape(BLK_DEV * NPB, PLEN, XW), grad_value.reshape(BLK_DEV * NPB, PLEN, XW))
    groups = (queries.reshape(N_ST, BLK_DEV, BLK, HEADS, HD), gate_pre.reshape(N_ST, BLK_DEV, BLK, HEADS, HD), cotangent.reshape(N_ST, BLK_DEV, BLK, HEADS, HD), passage_ids.reshape(N_ST, BLK_DEV, NPB))
    grad_queries, slot_keys, slot_values = lax.map(one_group, groups)
    grad_queries = grad_queries.reshape(TOKENS, XW)
    every_id = passage_ids.reshape(-1)
    passage_keys = jnp.zeros((PASSAGES, PLEN, XW), jnp.float32).at[every_id].add(slot_keys.reshape(BLOCKS * NPB, PLEN, XW))
    passage_values = jnp.zeros((PASSAGES, PLEN, XW), jnp.float32).at[every_id].add(slot_values.reshape(BLOCKS * NPB, PLEN, XW))
    passage_keys = passage_keys.astype(jnp.bfloat16).reshape(ROWS, XW)
    passage_values = passage_values.astype(jnp.bfloat16).reshape(ROWS, XW)
    grad_normed = jnp.dot(passage_keys, w_key.T, preferred_element_type=jnp.float32) + jnp.dot(passage_values, w_value.T, preferred_element_type=jnp.float32)
    grad_w_value = jnp.dot(normed.T, passage_values, preferred_element_type=jnp.float32)
    unit_rows = store_rows * row_inverse
    grad_unit = grad_normed * store_gain
    grad_store = row_inverse * (grad_unit - unit_rows * lax.optimization_barrier(jnp.mean(grad_unit * unit_rows, axis=-1, keepdims=True)))
    return (grad_queries, grad_store, grad_w_value)
```

```python
import functools

import jax
import jax.numpy as jnp
from jax import lax
from jax.experimental import pallas as pl
from jax.experimental.pallas import tpu as pltpu
from jax.sharding import PartitionSpec as P

HD = 128
PLEN = 64
EPS = 1e-06
NZ = 8
NJ = 8
NST = NZ * NJ
NTP = 4
MESH = pl.DeviceIdType.MESH
NT = (((1,), (1,)), ((), ()))
TN = (((0,), (0,)), ((), ()))
F32 = jnp.float32
BF16 = jnp.bfloat16


def dot(left, right, dims=(((1,), (0,)), ((), ()))):
    return lax.dot_general(left, right, dims, preferred_element_type=F32)


def row_scale(rows):
    return lax.rsqrt(jnp.mean(rows * rows, axis=-1, keepdims=True) + EPS)


def remote(src, dst, send_sem, recv_sem, axis, peer):
    return pltpu.make_async_remote_copy(
        src_ref=src, dst_ref=dst, send_sem=send_sem, recv_sem=recv_sem, device_id={axis: peer}, device_id_type=MESH
    )


def wait_bytes(ref, sem):
    pltpu.make_async_copy(ref, ref, sem).wait()


def greet(me, tp):
    z, j = me // NJ, me % NJ
    barrier = pltpu.get_barrier_semaphore()
    for t in range(1, NJ):
        pl.semaphore_signal(barrier, inc=1, device_id={"st": z * NJ + (j + t) % NJ}, device_id_type=MESH)
    for t in range(1, NZ):
        pl.semaphore_signal(barrier, inc=1, device_id={"st": (z + t) % NZ * NJ + j}, device_id_type=MESH)
    if tp is not None:
        for t in range(1, NTP):
            pl.semaphore_signal(barrier, inc=1, device_id={"tp": (tp + t) % NTP}, device_id_type=MESH)
    return barrier, NJ + NZ - 2 + (0 if tp is None else NTP - 1)


def table_kernel(owners, slots, store, gain, wk, wv, normed_out, kt, vt, meta, rows, normed, asked, in_sem, out_sem, ask_sem):
    me = lax.axis_index("st")
    z, j = me // NJ, me % NJ
    barrier, peers = greet(me, None)
    count = rows.shape[0] // 128

    def piece(i):
        return pl.ds(i * 128, 128)

    for i in range(count):
        pltpu.make_async_copy(store.at[piece(i)], rows.at[piece(i)], in_sem.at[i]).start()
    lane = lax.broadcasted_iota(jnp.int32, (1, 128), 1)
    request = jnp.full((1, 128), -1, jnp.int32)
    place = jnp.zeros((1, 128), jnp.int32)
    named = jnp.zeros((1, 128), jnp.int32)
    blocks, per_block = owners.shape
    for b in range(blocks):
        for i in range(per_block):
            at = b * per_block + i
            owner, slot = owners[b, i], slots[b, i]
            request = jnp.where(lane == owner, slot, request)
            place = jnp.where(lane == owner, at, place)
            named = jnp.where(lane == at, owner, named)
    asked[z, j] = request
    pl.semaphore_wait(barrier, peers)
    for t in range(1, NZ):
        far = (z + t) % NZ
        remote(asked.at[z, j], asked.at[z, j], ask_sem.at[0], ask_sem.at[1], "st", far * NJ + j).start()

    def project(i):
        at = piece(i)
        pltpu.make_async_copy(store.at[at], rows.at[at], in_sem.at[i]).wait()
        wide = rows[at].astype(F32)
        half = (wide * row_scale(wide) * gain[...]).astype(BF16)
        normed[at] = half
        kt[at] = dot(half, wk[...]).astype(BF16)
        vt[at] = dot(half, wv[...]).astype(BF16)
        pltpu.make_async_copy(normed.at[at], normed_out.at[at], out_sem.at[i]).start()

    for i in range(count // 2):
        project(i)
    wait_bytes(asked.at[pl.ds(0, NZ - 1), 0], ask_sem.at[1])
    for t in range(1, NJ):
        remote(asked.at[:, j], asked.at[:, j], ask_sem.at[2], ask_sem.at[3], "st", z * NJ + (j + t) % NJ).start()
    for i in range(count // 2, count):
        project(i)
    wait_bytes(asked.at[pl.ds(0, NJ - 1)], ask_sem.at[3])
    everyone = asked[...].reshape(NST, 128)
    lanes = lax.broadcasted_iota(jnp.int32, (NST, 128), 1)
    reader = lax.broadcasted_iota(jnp.int32, (NST, 128), 0)
    column = jnp.max(jnp.where(lanes == me, everyone, -1), axis=1, keepdims=True)
    across = jnp.max(jnp.where(lanes == reader, column, -1), axis=0, keepdims=True)
    before = jnp.max(jnp.where((reader < lanes) & (column == across), reader, -1), axis=0, keepdims=True)
    last = jnp.max(jnp.where(column == lanes, reader, -1), axis=0, keepdims=True)
    meta[0:1] = jnp.maximum(across, 0)
    meta[1:2] = jnp.where(before < 0, NST, before)
    meta[2:3] = jnp.where(last < 0, NST, last)
    meta[3:4] = place
    meta[4:5] = named
    meta[5:8] = jnp.zeros((3, 128), jnp.int32)
    wait_bytes(asked.at[pl.ds(0, NZ - 1), 0], ask_sem.at[0])
    wait_bytes(asked.at[pl.ds(0, NJ - 1)], ask_sem.at[2])
    for i in range(count):
        pltpu.make_async_copy(normed.at[piece(i)], normed_out.at[piece(i)], out_sem.at[i]).wait()


def tables(owners, slots, store, gain, w_key, w_value):
    rows, width = store.shape
    channels = w_key.shape[1]
    vmem = pl.BlockSpec(memory_space=pltpu.VMEM)
    smem = pl.BlockSpec(memory_space=pltpu.SMEM)
    far = pl.BlockSpec(memory_space=pltpu.HBM)
    return pl.pallas_call(
        table_kernel,
        out_shape=(
            jax.ShapeDtypeStruct((rows, width), BF16),
            jax.ShapeDtypeStruct((rows, channels), BF16),
            jax.ShapeDtypeStruct((rows, channels), BF16),
            jax.ShapeDtypeStruct((8, 128), jnp.int32),
        ),
        in_specs=[smem, smem, far, vmem, vmem, vmem],
        out_specs=(far, vmem, vmem, vmem),
        scratch_shapes=[
            pltpu.VMEM((rows, width), BF16),
            pltpu.VMEM((rows, width), BF16),
            pltpu.VMEM((NZ, NJ, 1, 128), jnp.int32),
            pltpu.SemaphoreType.DMA((rows // 128,)),
            pltpu.SemaphoreType.DMA((rows // 128,)),
            pltpu.SemaphoreType.DMA((4,)),
        ],
        cost_estimate=pl.CostEstimate(flops=3 * 10**9, bytes_accessed=10**7, transcendentals=0),
        compiler_params=pltpu.CompilerParams(collective_id=0, has_side_effects=True, vmem_limit_bytes=32 << 20),
        name="tables",
    )(owners, slots, store, gain, w_key, w_value)


TRANSIT = {(1, 2): 0, (1, 3): 8, (2, 3): 16, (1, 4): 24, (2, 4): 28, (3, 4): 32}
TRANSIT_PIECES = 36
ORDER = ((0, 4), (0, 3), (0, 2), (0, 1), (1, 4), (1, 3), (1, 2), (2, 4), (2, 3), (3, 4))


class Exchange:
    def __init__(self, me, number, x, column, transit, fin, z_send, z_recv, y_send, y_recv):
        self.z, self.j = me // NJ, me % NJ
        self.x, self.column, self.transit, self.fin = x, column.at[number], transit.at[number], fin
        self.z_send, self.z_recv = z_send.at[number], z_recv.at[number]
        self.y_send, self.y_recv = y_send.at[number], y_recv.at[number]

    def hop(self, side, g, d):
        s = 1 - 2 * side
        source = (self.z - s * g + NZ) % NZ
        dest = (source + s * d + NZ) % NZ
        first, count = (0, 8) if d < 4 else (4 * side, 4)
        if g == 0:
            src = self.x.at[pl.ds(dest * NJ + first, count)]
        else:
            src = self.transit.at[side, pl.ds(TRANSIT[g, d], count)]
        if g + 1 == d:
            dst = self.column.at[pl.ds(source * NJ + first, count)]
        else:
            dst = self.transit.at[side, pl.ds(TRANSIT[g + 1, d], count)]
        peer = (self.z + s + NZ) % NZ * NJ + self.j
        return remote(src, dst, self.z_send.at[side], self.z_recv.at[side, ORDER.index((g, d))], "st", peer)

    def send(self, *hops):
        for g, d in hops:
            for side in range(2):
                if g > 0:
                    self.hop(side, g - 1, d).wait_recv()
                self.hop(side, g, d).start()

    def spread(self, source, src):
        fin, z, j = self.fin, self.z, self.j
        pltpu.make_async_copy(src.at[source[0] * NJ + j], fin.at[source[1] * NJ + j], self.y_recv).start()

        @pl.loop(1, NJ)
        def _(t):
            other = (j + t) % NJ
            remote(src.at[source[0] * NJ + other], fin.at[source[1] * NJ + j], self.y_send, self.y_recv, "st", z * NJ + other).start()

    def spread_own(self):
        self.spread((self.z, self.z), self.x)

    def spread_from(self, d):
        for side in range(2):
            self.hop(side, d - 1, d).wait_recv()
        for side in range(1 if d == 4 else 2):
            source = (self.z - (1 - 2 * side) * d + NZ) % NZ
            self.spread((source, source), self.column)

    def arrive(self):
        wait_bytes(self.fin, self.y_recv)

    def finish(self):
        for side in range(2):
            wait_bytes(self.x, self.z_send.at[side])
        wait_bytes(self.fin.at[pl.ds(0, NZ * (NJ - 1))], self.y_send)


def main_kernel(
    meta, q_in, gate_in, cot_in, store_in, normed_in, wk_in, wv_in, gain, kt, vt,
    dq_ref, gs_ref, gw_ref,
    q, g, gate, x, column, transit, fin_k, fin_v, fin_b, weights, terms, stage, pv, wide_w, own, nrm, gwb, rs1, rsb, rs2, own_rows,
    z_send, z_recv, y_send, y_recv, in_sem, tp_sem, w_sem, rs_sem, nrm_sem,
):
    me = lax.axis_index("st")
    tp = lax.axis_index("tp")
    z, j = me // NJ, me % NJ
    core = me % 2
    scale = HD ** (-0.5)
    heads = q.shape[1] // HD
    width = q.shape[1]
    blocks = weights.shape[0]
    quarter = own.shape[1]
    barrier, peers = greet(me, tp)
    fins = (fin_k, fin_v, fin_b.at[0], fin_b.at[1])
    trips = [Exchange(me, n, x.at[n], column, transit, fins[n], z_send, z_recv, y_send, y_recv) for n in range(4)]
    ek, ev, bv, bk = trips
    mine = pl.ds(pl.multiple_of(tp * width, 128), width)

    loads = [
        pltpu.make_async_copy(q_in, q, in_sem.at[0]),
        pltpu.make_async_copy(cot_in, g, in_sem.at[1]),
        pltpu.make_async_copy(gate_in, gate, in_sem.at[2]),
        pltpu.make_async_copy(wk_in, wide_w.at[0, :, mine], in_sem.at[3]),
        pltpu.make_async_copy(wv_in, wide_w.at[1, :, mine], in_sem.at[4]),
        pltpu.make_async_copy(store_in.at[pl.ds(pl.multiple_of(tp * quarter, 16), quarter)], own_rows, in_sem.at[5]),
    ]
    for load in loads:
        load.start()

    def pick(table, number):
        @pl.loop(0, NST)
        def _(r):
            x[number, r] = table[meta[0, r]]

    pick(kt, 0)
    pl.semaphore_wait(barrier, peers)
    ek.send((0, 4), (0, 3), (0, 2), (0, 1))
    ek.spread_own()
    pick(vt, 1)

    part = wide_w.shape[1] // 2
    half = pl.ds(pl.multiple_of(core * part, 16), part)
    for load in loads[3:5]:
        load.wait()

    def weight_move(number, away):
        ref = wide_w.at[number, half, mine]
        return remote(ref, ref, w_sem.at[0, number, away], w_sem.at[1, number, away], "tp", (tp + away) % NTP)

    def weight_pass(number, away):
        ref = wide_w.at[number, half, pl.ds(pl.multiple_of((tp + NTP - away) % NTP * width, 128), width)]
        return remote(ref, ref, w_sem.at[2, number, away], w_sem.at[3, number, away], "st", me + 1 - 2 * core)

    for number in range(2):
        for away in range(1, NTP):
            weight_move(number, away).start()

    ek.send((1, 4), (1, 3), (1, 2))
    ek.spread_from(1)
    ek.send((2, 4), (2, 3))
    ek.spread_from(2)
    ev.send((0, 4), (0, 3))
    ek.send((3, 4))
    ev.send((0, 2), (0, 1))
    ev.spread_own()
    ek.spread_from(3)
    ek.spread_from(4)

    for load in loads[:3]:
        load.wait()

    @pl.loop(0, blocks)
    def _(b):
        at = pl.ds(b * 128, 128)
        g[at] = (jax.nn.sigmoid(gate[at].astype(F32)) * g[at].astype(F32)).astype(BF16)

    ek.arrive()

    def gathered(fin, b, cols):
        return jnp.concatenate([fin[meta[4, b * 4 + i], :, cols] for i in range(4)], axis=0)

    @pl.loop(0, blocks)
    def _(b):
        at = pl.ds(b * 128, 128)
        for h in range(heads):
            cols = pl.ds(h * HD, HD)
            score = dot(gathered(fin_k, b, cols), q[at, cols], NT) * scale
            raised = jnp.exp(score - jnp.max(score, axis=0, keepdims=True))
            weight = raised / jnp.sum(raised, axis=0, keepdims=True)
            weights[b, h] = weight
            terms[pl.ds(b * 4, 4), :, cols] = dot(weight.astype(BF16), g[at, cols]).astype(BF16).reshape(4, PLEN, HD)

    def order(number):
        @pl.loop(0, NST)
        def _(o):
            x[number, o] = terms[meta[3, o]]

    order(2)
    ev.send((1, 4), (1, 3), (1, 2))
    ev.spread_from(1)
    ev.send((2, 4), (2, 3))
    ev.spread_from(2)
    bv.send((0, 4), (0, 3))
    ev.send((3, 4))
    bv.send((0, 2), (0, 1))
    bv.spread_own()
    ev.spread_from(3)
    ev.spread_from(4)
    for number in range(2):
        for away in range(1, NTP):
            weight_move(number, away).wait_recv()
            weight_pass(number, away).start()
    ev.arrive()

    @pl.loop(0, blocks)
    def _(b):
        at = pl.ds(b * 128, 128)
        for h in range(heads):
            cols = pl.ds(h * HD, HD)
            steep = dot(gathered(fin_v, b, cols), g[at, cols], NT)
            weight = weights[b, h]
            delta = jnp.sum(weight.astype(BF16).astype(F32) * steep, axis=0, keepdims=True)
            slope = (weight * (steep - delta)).astype(BF16)
            terms[pl.ds(b * 4, 4), :, cols] = (dot(slope, q[at, cols]) * scale).astype(BF16).reshape(4, PLEN, HD)
            dq_ref[at, cols] = dot(slope, gathered(fin_k, b, cols), TN) * scale

    order(3)
    bv.send((1, 4), (1, 3), (1, 2))
    bv.spread_from(1)
    bv.send((2, 4), (2, 3))
    bv.spread_from(2)
    bk.send((0, 4), (0, 3))
    bv.send((3, 4))
    bk.send((0, 2), (0, 1))
    bk.spread_own()
    bv.spread_from(3)
    bv.spread_from(4)

    def normed_load(i):
        return pltpu.make_async_copy(normed_in.at[:, pl.ds(i * 256, 256)], nrm.at[i % 2], nrm_sem.at[i % 2])

    normed_load(0).start()
    stage[NST] = jnp.zeros(stage.shape[1:], F32)
    bv.arrive()

    def add_up(fin):
        for h in range(heads):
            cols = pl.ds(h * HD, HD)

            @pl.loop(0, NST)
            def _(r):
                stage[r] = fin[r, :, cols].astype(F32) + stage[meta[1, r]]

            @pl.loop(0, pv.shape[0] // PLEN)
            def _(p):
                pv[pl.ds(pl.multiple_of(p * PLEN, PLEN), PLEN), cols] = stage[meta[2, p]].astype(BF16)

    def across(number, away):
        src = pv.at[pl.ds(pl.multiple_of((tp + away) % NTP * quarter, 16), quarter)]
        return remote(src, own.at[number, :, mine], tp_sem.at[0, number, away], tp_sem.at[1, number, away], "tp", (tp + away) % NTP)

    def kept(number):
        src = pv.at[pl.ds(pl.multiple_of(tp * quarter, 16), quarter)]
        return pltpu.make_async_copy(src, own.at[number, :, mine], tp_sem.at[0, number, 0])

    add_up(fins[2])
    kept(1).start()
    for away in range(1, NTP):
        across(1, away).start()
    bk.send((1, 4), (1, 3), (1, 2))
    bk.spread_from(1)
    for i in range(NZ):
        if i + 1 < NZ:
            normed_load(i + 1).start()
        normed_load(i).wait()
        gwb[i] = dot(nrm[i % 2], pv[...], TN).astype(BF16).reshape(NJ, 32, width)
    for t in range(1, NJ):
        other = (j + t) % NJ
        remote(gwb.at[:, other], rs1.at[j], rs_sem.at[0], rs_sem.at[1], "st", z * NJ + other).start()
    bk.send((2, 4), (2, 3))
    bk.spread_from(2)
    bk.send((3, 4))
    wait_bytes(rs1.at[pl.ds(0, NJ - 1)], rs_sem.at[1])
    total = gwb[:, j].astype(F32)
    for t in range(1, NJ):
        total = total + rs1[(j + t) % NJ].astype(F32)
    rsb[...] = total.astype(BF16)
    gw_ref[...] = gwb[z, j].astype(F32)
    for t in range(1, NJ):
        gw_ref[...] += rs1[(j + t) % NJ, z].astype(F32)
    bk.spread_from(3)
    for t in range(1, NZ):
        other = (z + t) % NZ
        remote(rsb.at[other], rs2.at[z], rs_sem.at[2], rs_sem.at[3], "st", other * NJ + j).start()
    bk.spread_from(4)
    for number in range(2):
        for away in range(1, NTP):
            weight_pass(number, away).wait_recv()
    kept(1).wait()
    for away in range(1, NTP):
        across(1, away).wait()
    for i in range(8):
        out = pl.ds(i * 256, 256)
        gs_ref[:, out] = dot(own[1], wide_w[1, out], NT)
    wait_bytes(rs2.at[pl.ds(0, NZ - 1)], rs_sem.at[3])
    for t in range(1, NZ):
        gw_ref[...] += rs2[(z + t) % NZ].astype(F32)
    loads[5].wait()
    bk.arrive()
    add_up(fins[3])
    kept(0).start()
    for away in range(1, NTP):
        across(0, away).start()
    kept(0).wait()
    for away in range(1, NTP):
        across(0, away).wait()
    for i in range(8):
        out = pl.ds(i * 256, 256)
        gs_ref[:, out] += dot(own[0], wide_w[0, out], NT)

    @pl.loop(0, quarter // 32)
    def _(i):
        at = pl.ds(pl.multiple_of(i * 32, 32), 32)
        rows = own_rows[at].astype(F32)
        inverse = row_scale(rows)
        unit = rows * inverse
        grad_unit = gs_ref[at] * gain[...]
        gs_ref[at] = inverse * (grad_unit - unit * jnp.mean(grad_unit * unit, axis=-1, keepdims=True))

    for trip in trips:
        trip.finish()
    for number in range(2):
        for away in range(1, NTP):
            weight_move(number, away).wait_send()
            weight_pass(number, away).wait_send()
    wait_bytes(rs1.at[pl.ds(0, NJ - 1)], rs_sem.at[0])
    wait_bytes(rs2.at[pl.ds(0, NZ - 1)], rs_sem.at[2])


def attend(meta, queries, gate_pre, cotangent, store, normed, w_key, w_value, gain, key_table, value_table):
    tokens, width = queries.shape
    rows, features = store.shape
    heads = width // HD
    blocks = tokens // 128
    quarter = rows // NTP
    vmem = pl.BlockSpec(memory_space=pltpu.VMEM)
    smem = pl.BlockSpec(memory_space=pltpu.SMEM)
    far = pl.BlockSpec(memory_space=pltpu.HBM)
    piece = (PLEN, width)
    dma = pltpu.SemaphoreType.DMA
    return pl.pallas_call(
        main_kernel,
        out_shape=(
            jax.ShapeDtypeStruct((tokens, width), F32),
            jax.ShapeDtypeStruct((quarter, features), F32),
            jax.ShapeDtypeStruct((features // NST, width), F32),
        ),
        in_specs=[smem] + [far] * 7 + [vmem] * 3,
        out_specs=(vmem,) * 3,
        scratch_shapes=[
            pltpu.VMEM((tokens, width), BF16),
            pltpu.VMEM((tokens, width), BF16),
            pltpu.VMEM((tokens, width), BF16),
            pltpu.VMEM((4, NST) + piece, BF16),
            pltpu.VMEM((4, NST) + piece, BF16),
            pltpu.VMEM((4, 2, TRANSIT_PIECES) + piece, BF16),
            pltpu.VMEM((NST,) + piece, BF16),
            pltpu.VMEM((NST,) + piece, BF16),
            pltpu.VMEM((2, NST) + piece, BF16),
            pltpu.VMEM((blocks, heads, 256, 128), F32),
            pltpu.VMEM((blocks * 4,) + piece, BF16),
            pltpu.VMEM((NST + 1, PLEN, HD), F32),
            pltpu.VMEM((rows, width), BF16),
            pltpu.VMEM((2, features, width * NTP), BF16),
            pltpu.VMEM((2, quarter, width * NTP), BF16),
            pltpu.VMEM((2, rows, 256), BF16),
            pltpu.VMEM((NZ, NJ, features // NST, width), BF16),
            pltpu.VMEM((NJ, NZ, features // NST, width), BF16),
            pltpu.VMEM((NZ, features // NST, width), BF16),
            pltpu.VMEM((NZ, features // NST, width), BF16),
            pltpu.VMEM((quarter, features), BF16),
            dma((4, 2)),
            dma((4, 2, len(ORDER))),
            dma((4,)),
            dma((4,)),
            dma((6,)),
            dma((2, 2, NTP)),
            dma((4, 2, NTP)),
            dma((4,)),
            dma((2,)),
        ],
        cost_estimate=pl.CostEstimate(flops=10**10, bytes_accessed=10**7, transcendentals=0),
        compiler_params=pltpu.CompilerParams(collective_id=1, has_side_effects=True, vmem_limit_bytes=67043328),
        name="attend",
    )(meta, queries, gate_pre, cotangent, store, normed, w_key, w_value, gain, key_table, value_table)


def local(queries, gate_pre, cotangent, store, store_gain, w_key, w_value, owners, slots):
    gain = store_gain[None]
    normed, key_table, value_table, meta = tables(owners, slots, store, gain, w_key, w_value)
    key_table, value_table = (table.reshape(-1, PLEN, table.shape[1]) for table in (key_table, value_table))
    grad_queries, grad_store, grad_w_value = attend(
        meta, queries, gate_pre, cotangent, store, normed, w_key, w_value, gain, key_table, value_table
    )
    return (grad_queries, grad_store, grad_w_value)


def solution(mesh):
    placed = (
        P("st", "tp"),
        P("st", "tp"),
        P("st", "tp"),
        P("st", None),
        P(),
        P(None, "tp"),
        P(None, "tp"),
        P("st", None),
        P("st", None),
    )
    return jax.shard_map(
        local,
        mesh=mesh,
        in_specs=placed,
        out_specs=(P("st", "tp"), P(("st", "tp"), None), P("st", "tp")),
        check_vma=False,
    )
```

```python
import functools

import jax
import jax.numpy as jnp
from jax import lax
from jax.experimental import pallas as pl
from jax.experimental.pallas import tpu as pltpu
from jax.sharding import PartitionSpec as P

HD = 128
PLEN = 64
EPS = 1e-06
NZ = 8
NJ = 8
NST = NZ * NJ
NTP = 4
MESH = pl.DeviceIdType.MESH
NT = (((1,), (1,)), ((), ()))
TN = (((0,), (0,)), ((), ()))
F32 = jnp.float32
BF16 = jnp.bfloat16


def dot(left, right, dims=(((1,), (0,)), ((), ()))):
    return lax.dot_general(left, right, dims, preferred_element_type=F32)


def row_scale(rows):
    return lax.rsqrt(jnp.mean(rows * rows, axis=-1, keepdims=True) + EPS)


def remote(src, dst, send_sem, recv_sem, axis, peer):
    return pltpu.make_async_remote_copy(
        src_ref=src, dst_ref=dst, send_sem=send_sem, recv_sem=recv_sem, device_id={axis: peer}, device_id_type=MESH
    )


def wait_bytes(ref, sem):
    pltpu.make_async_copy(ref, ref, sem).wait()


def greet(me, tp):
    z, j = me // NJ, me % NJ
    barrier = pltpu.get_barrier_semaphore()
    for t in range(1, NJ):
        pl.semaphore_signal(barrier, inc=1, device_id={"st": z * NJ + (j + t) % NJ}, device_id_type=MESH)
    for t in range(1, NZ):
        pl.semaphore_signal(barrier, inc=1, device_id={"st": (z + t) % NZ * NJ + j}, device_id_type=MESH)
    if tp is not None:
        for t in range(1, NTP):
            pl.semaphore_signal(barrier, inc=1, device_id={"tp": (tp + t) % NTP}, device_id_type=MESH)
    return barrier, NJ + NZ - 2 + (0 if tp is None else NTP - 1)


NY = NJ // 2


PASSAGES = 20
PART = PASSAGES // 2
BASE = 24
PREV, LAST, PLACE, NAMED, META_ROWS = 64, 68, 72, 73, 80


class Column:
    def __init__(self, me, via, z_send, z_recv, y_send, y_recv, via_send, via_recv):
        self.z, self.j, self.long, self.via = me // NJ, me % NJ, 1 - 2 * (me % 2), via
        self.z_send, self.z_recv, self.y_send, self.y_recv = z_send, z_recv, y_send, y_recv
        self.via_send, self.via_recv = via_send, via_recv

    def plane(self, steps):
        return (self.z + steps * self.long + NZ) % NZ

    def step(self, side, number, src, dst):
        peer = self.plane(1 - 2 * side) * NJ + self.j
        return remote(src, dst, self.z_send.at[side], self.z_recv.at[number], "st", peer)

    def beside(self, steps, core):
        return (self.j // 2 + steps + NY) % NY * 2 + core

    def spread(self, src, dst, plane, recv_sem):
        z, j, core = self.z, self.j, self.j % 2
        pltpu.make_async_copy(src.at[plane * NJ + j], dst.at[plane * NJ + j], recv_sem).start()
        for way in range(2):
            peer = z * NJ + self.beside(1 - 2 * way, core)
            ref = src.at[plane * NJ + self.beside(2, way)]
            remote(ref, self.via.at[2 * plane + way], self.y_send, self.via_recv.at[2 * plane + way], "st", peer).start()
        for steps, to in ((1, 0), (1, 1), (-1, 0), (-1, 1), (0, 1 - core)):
            other = self.beside(steps, to)
            remote(src.at[plane * NJ + other], dst.at[plane * NJ + j], self.y_send, recv_sem, "st", z * NJ + other).start()

    def pass_on(self, dst, plane, recv_sem):
        for way in range(2):
            steps = 1 - 2 * way
            ref = self.via.at[2 * plane + way]
            wait_bytes(ref, self.via_recv.at[2 * plane + way])
            place = plane * NJ + self.beside(-steps, self.j % 2)
            remote(ref, dst.at[place], self.via_send, recv_sem, "st", self.z * NJ + self.beside(steps, way)).start()


class Outward(Column):
    def __init__(self, me, meta, table, near, far, picked, passed, column, fin, via, *sems):
        super().__init__(me, via, *sems)
        self.meta, self.table, self.near, self.far = meta, table, near, far
        self.picked, self.passed, self.column, self.fin = picked, passed, column, fin

    def launch(self, part, side):
        at = pl.ds(part * PART, PART)
        return self.step(side, 2 * side + part, self.table.at[at], self.near.at[side, at])

    def relay(self, part):
        at = pl.ds(part * PART, PART)
        return self.step(0, 4 + part, self.near.at[0, at], self.far.at[at])

    def hop(self, name):
        column, picked, passed, at = self.column, self.picked, self.passed, self.block
        return {
            "s2": lambda: self.step(1, 6, picked.at[0], column.at[at(self.plane(1))]),
            "s3": lambda: self.step(1, 7, picked.at[1], passed.at[1]),
            "s3b": lambda: self.step(1, 8, passed.at[1], column.at[at(self.plane(2))]),
            "l3": lambda: self.step(0, 9, picked.at[2], column.at[at(self.plane(-2))]),
            "l4": lambda: self.step(0, 10, picked.at[3], passed.at[0]),
            "l4b": lambda: self.step(0, 11, passed.at[0], column.at[at(self.plane(-3))]),
        }[name]()

    def block(self, plane):
        return pl.ds(plane * NJ, NJ)

    def pick(self, table, owner_plane, reader_plane, out, first):
        meta, owner = self.meta, owner_plane * NJ + self.j

        @pl.loop(0, NJ)
        def _(t):
            out[first + t] = table[jnp.maximum(meta[reader_plane * NJ + t, owner], 0)]

    def deliver(self, plane):
        self.spread(self.column, self.fin, plane, self.y_recv.at[0])

    def onward(self, *steps):
        for one in steps:
            self.pass_on(self.fin, self.plane(one), self.y_recv.at[0])

    def start(self, part):
        for side in range(2):
            self.launch(part, side).start()

    def own(self):
        self.pick(self.table, self.z, self.z, self.column, self.z * NJ)
        self.deliver(self.z)

    def first(self):
        for part in range(2):
            self.launch(part, 0).wait_recv()
            self.relay(part).start()
        for part in range(2):
            self.launch(part, 1).wait_recv()
        owner = self.plane(1)
        self.pick(self.near.at[1], owner, self.plane(-2), self.picked.at[1], 0)
        self.hop("s3").start()
        self.pick(self.near.at[1], owner, self.plane(-1), self.picked.at[0], 0)
        self.hop("s2").start()
        for owner, side in ((self.plane(-1), 0), (self.plane(1), 1)):
            self.pick(self.near.at[side], owner, self.z, self.column, owner * NJ)
            self.deliver(owner)

    def second(self):
        self.hop("s3").wait_recv()
        self.hop("s3b").start()
        for part in range(2):
            self.relay(part).wait_recv()
        owner = self.plane(-2)
        self.pick(self.far, owner, self.plane(2), self.picked.at[3], 0)
        self.hop("l4").start()
        self.pick(self.far, owner, self.plane(1), self.picked.at[2], 0)
        self.hop("l3").start()
        self.pick(self.far, owner, self.z, self.column, owner * NJ)
        self.deliver(owner)
        self.hop("s2").wait_recv()
        self.deliver(self.plane(2))

    def third(self):
        self.hop("l4").wait_recv()
        self.hop("l4b").start()
        self.hop("s3b").wait_recv()
        self.deliver(self.plane(3))
        self.hop("l3").wait_recv()
        self.deliver(self.plane(-3))

    def fourth(self):
        self.hop("l4b").wait_recv()
        self.deliver(self.plane(-4))

    def arrive(self):
        wait_bytes(self.fin, self.y_recv.at[0])

    def finish(self):
        wait_bytes(self.column, self.z_send.at[0])
        wait_bytes(self.column.at[pl.ds(0, 44)], self.z_send.at[1])
        wait_bytes(self.column.at[pl.ds(0, NZ * (NJ - 1))], self.y_send)
        wait_bytes(self.via, self.via_send)


class Homeward(Column):
    def __init__(self, me, meta, x, column, slots, sums, gained, stage, via, *sems):
        super().__init__(me, via, *sems)
        self.meta, self.x, self.column, self.slots = meta, x, column, slots
        self.sums, self.gained, self.stage = sums, gained, stage

    def block(self, plane):
        return pl.ds(plane * NJ, NJ)

    def hop(self, name):
        mine = lambda steps: self.column.at[self.block(self.plane(steps))]
        slots, sums, gained = self.slots, self.sums, self.gained
        return {
            "l4": lambda: self.step(1, 0, mine(-4), slots.at[0]),
            "l3": lambda: self.step(1, 1, mine(-3), slots.at[1]),
            "l4b": lambda: self.step(1, 2, slots.at[0], slots.at[2]),
            "l2": lambda: self.step(1, 3, sums.at[0], gained.at[0]),
            "l1": lambda: self.step(1, 4, sums.at[1], gained.at[1]),
            "s3": lambda: self.step(0, 5, mine(3), slots.at[3]),
            "s2": lambda: self.step(0, 6, mine(2), slots.at[4]),
            "s3b": lambda: self.step(0, 7, slots.at[3], slots.at[5]),
            "s1": lambda: self.step(0, 8, sums.at[2], gained.at[2]),
        }[name]()

    def start(self, *steps):
        for one in steps:
            plane = self.plane(one)
            self.spread(self.x, self.column, plane, self.y_recv.at[plane])

    def onward(self, *steps):
        for one in steps:
            plane = self.plane(one)
            self.pass_on(self.column, plane, self.y_recv.at[plane])

    def gathered(self, steps):
        plane = self.plane(steps)
        wait_bytes(self.column.at[self.block(plane)], self.y_recv.at[plane])

    def add_up(self, combo, planes, slots, bases, store):
        meta, stage = self.meta, self.stage
        width = self.x.shape[-1]
        for first in range(0, width, HD):
            cols = pl.ds(first, HD)

            @pl.loop(0, PASSAGES)
            def _(p):
                total = jnp.zeros(stage.shape[1:], F32)
                for base in bases:
                    total = total + base[p, :, cols].astype(F32)
                stage[BASE + p] = total

            for rank, (plane, (ref, start)) in enumerate(zip(planes, slots)):

                @pl.loop(0, NJ)
                def _(t):
                    stage[rank * NJ + t] = ref[start + t, :, cols].astype(F32) + stage[meta[PREV + combo, plane * NJ + t]]

            @pl.loop(0, PASSAGES)
            def _(p):
                store(p, cols, stage[meta[LAST + combo, p]].astype(BF16))

    def into(self, number):
        def store(p, cols, value):
            self.sums[number, p, :, cols] = value

        return store

    def first(self):
        self.gathered(-4)
        self.hop("l4").start()
        self.gathered(3)
        self.hop("s3").start()
        self.gathered(-3)
        self.hop("l3").start()
        self.gathered(2)
        self.hop("s2").start()

    def second(self):
        self.hop("l4").wait_recv()
        self.hop("l4b").start()
        self.hop("s3").wait_recv()
        self.hop("s3b").start()

    def third(self):
        self.gathered(-2)
        self.hop("l3").wait_recv()
        self.hop("l4b").wait_recv()
        planes = (self.plane(2), self.plane(1), self.z)
        slots = ((self.slots.at[2], 0), (self.slots.at[1], 0), (self.column, self.plane(-2) * NJ))
        self.add_up(0, planes, slots, (), self.into(0))
        self.hop("l2").start()
        self.gathered(1)
        self.hop("s2").wait_recv()
        self.hop("s3b").wait_recv()
        planes = (self.plane(-2), self.plane(-1), self.z)
        slots = ((self.slots.at[5], 0), (self.slots.at[4], 0), (self.column, self.plane(1) * NJ))
        self.add_up(2, planes, slots, (), self.into(2))
        self.hop("s1").start()

    def fourth(self):
        self.gathered(-1)
        self.hop("l2").wait_recv()
        slots = ((self.column, self.plane(-1) * NJ),)
        self.add_up(1, (self.z,), slots, (self.gained.at[0],), self.into(1))
        self.hop("l1").start()

    def collect(self, store):
        self.gathered(0)
        self.hop("l1").wait_recv()
        self.hop("s1").wait_recv()
        slots = ((self.column, self.z * NJ),)
        self.add_up(3, (self.z,), slots, (self.gained.at[1], self.gained.at[2]), store)

    def finish(self):
        wait_bytes(self.column, self.z_send.at[1])
        wait_bytes(self.column.at[pl.ds(0, 44)], self.z_send.at[0])
        wait_bytes(self.column.at[pl.ds(0, NZ * (NJ - 1))], self.y_send)
        wait_bytes(self.via, self.via_send)


def plans(asked, me, place, named, meta):
    z, j, long = me // NJ, me % NJ, 1 - 2 * (me % 2)
    everyone = asked[...].reshape(NST, 128)
    meta[0:NST] = everyone
    lanes = lax.broadcasted_iota(jnp.int32, (NST, 128), 1)
    reader = lax.broadcasted_iota(jnp.int32, (NST, 128), 0)
    combos = ((-2, 2, 3, -1), (-1, 0, 1, -1), (1, -2, 3, 1), (0, 0, 1, 1))
    for number, (owner, start, count, way) in enumerate(combos):
        owner = (z + owner * long + NZ) % NZ * NJ + j
        start = (z + start * long + NZ) % NZ

        def rank(index):
            return ((index // NJ - start) * (way * long) + 2 * NZ) % NZ * NJ + index % NJ

        mine, other = rank(reader), rank(lanes)
        column = jnp.max(jnp.where(lanes == owner, everyone, -1), axis=1, keepdims=True)
        across = jnp.max(jnp.where(lanes == reader, column, -1), axis=0, keepdims=True)
        inside = mine < count * NJ
        before = jnp.max(jnp.where(inside & (mine < other) & (column == across), mine, -1), axis=0, keepdims=True)
        last = jnp.max(jnp.where(inside & (column == lanes), mine, -1), axis=0, keepdims=True)
        spot = lax.broadcasted_iota(jnp.int32, (1, 128), 1)
        meta[PREV + number : PREV + number + 1] = jnp.where(before < 0, BASE + jnp.maximum(across, 0), before)
        meta[LAST + number : LAST + number + 1] = jnp.where(last < 0, BASE + spot, last)
    meta[PLACE : PLACE + 1] = place
    meta[NAMED : NAMED + 1] = named
    meta[NAMED + 1 : META_ROWS] = jnp.zeros((META_ROWS - NAMED - 1, 128), jnp.int32)


def kernel(
    owners, slots, q_in, gate_in, cot_in, store_in, wk_in, wv_in, gain,
    dq_out, gs_out, gw_ref,
    rows, tables, asked, plan, meta, q, g, near_k, near_v, far_k, far_v, picked, passed, out_column, out_via, fin_k, fin_v, x, column, via_v, slot_v, sum_v, gain_v,
    xk, columnk, via_k, slot_k, sum_k, gain_k, weights, terms, stage, pv, pk, wide_w, own, gwb, rs1, rsb, rs2, gs,
    oz_send, oz_recv, oy_send, oy_recv, ov_send, ov_recv, hz_send, hz_recv, hy_send, hy_recv, hv_send, hv_recv,
    row_sem, ask_sem, in_sem, tp_sem, w_sem, rs_sem, out_sem,
):
    me = lax.axis_index("st")
    tp = lax.axis_index("tp")
    z, j = me // NJ, me % NJ
    core = me % 2
    scale = HD ** (-0.5)
    heads = q.shape[1] // HD
    width = q.shape[1]
    blocks = weights.shape[0]
    quarter = gs.shape[0]
    barrier, peers = greet(me, tp)
    slim = pl.ds(pl.multiple_of(tp * HD, HD), HD)

    def out_sems(n):
        return oz_send.at[n], oz_recv.at[n], oy_send.at[n], oy_recv.at[n], ov_send.at[n], ov_recv.at[n]

    def home_sems(n):
        return hz_send.at[n], hz_recv.at[n], hy_send.at[n], hy_recv.at[n], hv_send.at[n], hv_recv.at[n]

    fins = (fin_k, fin_v)
    ek, ev = (
        Outward(me, meta, tables.at[n], (near_k, near_v)[n], (far_k, far_v)[n], picked.at[n], passed.at[n], out_column.at[n], fins[n], out_via.at[n], *out_sems(n))
        for n in range(2)
    )
    bv = Homeward(me, meta, x, column, slot_v, sum_v, gain_v, stage, via_v, *home_sems(0))
    bk = [
        Homeward(me, meta, xk.at[h], columnk.at[h], slot_k.at[h], sum_k.at[h], gain_k.at[h], stage, via_k.at[h], *home_sems(1 + h))
        for h in range(2)
    ]

    weight_loads = [
        pltpu.make_async_copy(ref.at[:, :, pl.ds(h * HD, HD)], wide_w.at[n, h, :, :, slim], in_sem.at[2 * n + h])
        for n, ref in enumerate((wk_in, wv_in))
        for h in range(2)
    ]
    first_loads = [
        pltpu.make_async_copy(ref, x.at[pl.ds(n * NST // 2, NST // 2)], in_sem.at[7 + n])
        for n, ref in enumerate((wk_in, wv_in))
    ]
    token_loads = [
        pltpu.make_async_copy(q_in, q, in_sem.at[4]),
        pltpu.make_async_copy(cot_in, g, in_sem.at[5]),
        pltpu.make_async_copy(gate_in, pv.at[pl.ds(0, gate_in.shape[0])], in_sem.at[6]),
    ]
    count = rows.shape[0] // 256

    def chunk(i):
        return pl.ds(i * 256, 256)

    def row_load(i):
        return pltpu.make_async_copy(store_in.at[chunk(i)], rows.at[chunk(i)], row_sem.at[i])

    row_load(0).start()
    for load in first_loads:
        load.start()
    for i in range(1, count):
        row_load(i).start()
    for load in weight_loads + token_loads:
        load.start()

    lane = lax.broadcasted_iota(jnp.int32, (1, 128), 1)
    request = jnp.full((1, 128), -1, jnp.int32)
    place = jnp.zeros((1, 128), jnp.int32)
    named = jnp.zeros((1, 128), jnp.int32)
    per_block = owners.shape[0]
    for b in range(blocks):
        for i in range(per_block):
            at = b * per_block + i
            owner, slot = owners[i, b], slots[i, b]
            request = jnp.where(lane == owner, slot, request)
            place = jnp.where(lane == owner, at, place)
            named = jnp.where(lane == at, owner, named)
    asked[z, j] = request
    for load in first_loads:
        load.wait()

    def project(i):
        at = chunk(i)
        row_load(i).wait()

        @pl.loop(0, 8)
        def _(t):
            tile = pl.ds(i * 256 + t * 32, 32)
            raw = rows[tile].astype(F32)
            rows[tile] = (raw * row_scale(raw) * gain[...]).astype(BF16)

        for n in range(2):
            weight = x[pl.ds(n * NST // 2, NST // 2)].reshape(rows.shape[1], width)
            tables[n, pl.ds(4 * i, 4)] = dot(rows[at], weight).astype(BF16).reshape(4, PLEN, width)

    project(0)
    project(1)
    project(2)
    pl.semaphore_wait(barrier, peers)
    for t in range(1, NZ):
        other = (z + t) % NZ
        remote(asked.at[z, j], asked.at[z, j], ask_sem.at[0], ask_sem.at[1], "st", other * NJ + j).start()
    ek.start(0)
    project(3)
    project(4)
    ek.start(1)
    wait_bytes(asked.at[pl.ds(0, NZ - 1), 0], ask_sem.at[1])
    for t in range(1, NJ):
        remote(asked.at[:, j], asked.at[:, j], ask_sem.at[2], ask_sem.at[3], "st", z * NJ + (j + t) % NJ).start()
    ev.start(0)
    ev.start(1)

    part = wide_w.shape[2] // 2
    half_rows = pl.ds(core * part, part)

    def weight_move(n, away):
        ref = wide_w.at[n, :, half_rows, :, slim]
        return remote(ref, ref, w_sem.at[0, n, away], w_sem.at[1, n, away], "tp", (tp + away) % NTP)

    def weight_pass(n, away):
        ref = wide_w.at[n, :, half_rows, :, pl.ds(pl.multiple_of((tp + NTP - away) % NTP * HD, HD), HD)]
        return remote(ref, ref, w_sem.at[2, n, away], w_sem.at[3, n, away], "st", me + 1 - 2 * core)

    for load in weight_loads:
        load.wait()
    for n in range(2):
        for away in range(1, NTP):
            weight_move(n, away).start()
    wait_bytes(asked.at[pl.ds(0, NJ - 1)], ask_sem.at[3])
    plans(asked, me, place, named, plan)
    sent_plan = pltpu.make_async_copy(plan, meta, ask_sem.at[4])
    sent_plan.start()
    for load in token_loads:
        load.wait()

    @pl.loop(0, blocks)
    def _(b):
        at = pl.ds(b * 128, 128)
        g[at] = (jax.nn.sigmoid(pv[at].astype(F32)) * g[at].astype(F32)).astype(BF16)

    sent_plan.wait()
    ek.own()
    ek.first()
    ev.own()
    ek.onward(0, -1, 1)
    ek.second()
    ev.onward(0)
    ev.first()
    ek.onward(-2, 2)
    ek.third()
    ek.onward(3, -3)
    ek.fourth()
    ev.onward(-1, 1)
    ek.onward(-4)
    ek.arrive()

    def joined(n, b, cols):
        return jnp.concatenate([fins[n][meta[NAMED, b * 4 + i], :, cols] for i in range(4)], axis=0)

    @pl.loop(0, blocks)
    def _(b):
        at = pl.ds(b * 128, 128)
        for h in range(heads):
            cols = pl.ds(h * HD, HD)
            score = dot(joined(0, b, cols), q[at, cols], NT) * scale
            raised = jnp.exp(score - jnp.max(score, axis=0, keepdims=True))
            weight = raised / jnp.sum(raised, axis=0, keepdims=True)
            weight = weight.astype(BF16)
            weights[b, h] = weight
            terms[pl.ds(b * 4, 4), :, cols] = dot(weight, g[at, cols]).astype(BF16).reshape(4, PLEN, HD)

    @pl.loop(0, NST)
    def _(o):
        x[o] = terms[meta[PLACE, o]]

    bv.start(-4, 3, -3, 2, -2)
    ev.second()
    bv.onward(-4, 3, -3, 2, -2)
    ev.onward(-2, 2)
    ev.third()
    bv.first()
    ev.onward(3, -3)
    ev.fourth()
    bv.second()
    ev.onward(-4)
    bv.start(1, -1, 0)
    for n in range(2):
        for away in range(1, NTP):
            weight_move(n, away).wait_recv()
            weight_pass(n, away).start()
    ev.arrive()

    @pl.loop(0, blocks)
    def _(b):
        at = pl.ds(b * 128, 128)
        for h in range(heads):
            cols = pl.ds(h * HD, HD)
            steep = dot(joined(1, b, cols), g[at, cols], NT)
            weight = weights[b, h].astype(F32)
            delta = jnp.sum(weight * steep, axis=0, keepdims=True)
            slope = (weight * (steep - delta)).astype(BF16)
            terms[pl.ds(b * 4, 4), :, cols] = (dot(slope, q[at, cols]) * scale).astype(BF16).reshape(4, PLEN, HD)
            q[at, cols] = (dot(slope, joined(0, b, cols), TN) * scale).astype(BF16)

    dq_store = pltpu.make_async_copy(q, dq_out, out_sem.at[0])
    dq_store.start()

    @pl.loop(0, NST)
    def _(o):
        for h in range(2):
            xk[h, o] = terms[meta[PLACE, o], :, pl.ds(h * HD, HD)]

    bv.onward(1, -1, 0)
    bk[0].start(-4, 3, -3, 2, -2)
    bv.third()
    bk[0].onward(-4, 3, -3, 2, -2)
    bk[0].first()
    bk[0].start(1, -1, 0)
    bk[1].start(-4, 3, -3, 2, -2)
    bv.fourth()
    bk[0].onward(1, -1, 0)
    bk[1].onward(-4, 3, -3, 2, -2)
    bk[0].second()
    bk[1].first()
    bk[1].start(1, -1, 0)

    def keep(ref):
        def store(p, cols, value):
            ref[pl.ds(pl.multiple_of(p * PLEN, PLEN), PLEN), cols] = value

        return store

    bv.collect(keep(pv))

    def across(n, away):
        src = (pk.at[0], pk.at[1], pv.at[:, pl.ds(0, HD)], pv.at[:, pl.ds(HD, HD)])[n]
        peer = (tp + away) % NTP
        at = pl.ds(pl.multiple_of(peer * quarter, 16), quarter)
        return remote(src.at[at], own.at[n, :, slim], tp_sem.at[0, n, away], tp_sem.at[1, n, away], "tp", peer)

    def kept(n):
        src = (pk.at[0], pk.at[1], pv.at[:, pl.ds(0, HD)], pv.at[:, pl.ds(HD, HD)])[n]
        return pltpu.make_async_copy(src.at[pl.ds(pl.multiple_of(tp * quarter, 16), quarter)], own.at[n, :, slim], tp_sem.at[0, n, 0])

    def exchange(n):
        kept(n).start()
        for away in range(1, NTP):
            across(n, away).start()

    def exchanged(n):
        kept(n).wait()
        for away in range(1, NTP):
            across(n, away).wait()

    def weight_rows(n, h, i):
        return wide_w[n, h, 4 * i : 4 * i + 4].reshape(256, HD * NTP)

    exchange(2)
    exchange(3)
    bk[0].third()
    bk[1].onward(1, -1, 0)
    bk[1].second()
    for i in range(NZ):
        gwb[i] = dot(rows[:, i * 256 : (i + 1) * 256], pv[...], TN).astype(BF16).reshape(NJ, 32, width)
    own_rows = pltpu.make_async_copy(
        store_in.at[pl.ds(pl.multiple_of(tp * quarter, 16), quarter)], rows.at[pl.ds(0, quarter)], out_sem.at[1]
    )
    own_rows.start()
    for t in range(1, NJ):
        other = (j + t) % NJ
        remote(gwb.at[:, other], rs1.at[j], rs_sem.at[0], rs_sem.at[1], "st", z * NJ + other).start()
    bk[0].fourth()
    bk[1].third()
    wait_bytes(rs1.at[pl.ds(0, NJ - 1)], rs_sem.at[1])
    total = gwb[:, j].astype(F32)
    for t in range(1, NJ):
        total = total + rs1[(j + t) % NJ].astype(F32)
    rsb[...] = total.astype(BF16)
    gw_ref[...] = gwb[z, j].astype(F32)
    for t in range(1, NJ):
        gw_ref[...] += rs1[(j + t) % NJ, z].astype(F32)
    for t in range(1, NZ):
        other = (z + t) % NZ
        remote(rsb.at[other], rs2.at[z], rs_sem.at[2], rs_sem.at[3], "st", other * NJ + j).start()
    bk[0].collect(keep(pk.at[0]))
    exchange(0)
    bk[1].fourth()
    for n in range(2):
        for away in range(1, NTP):
            weight_pass(n, away).wait_recv()
    exchanged(2)
    exchanged(3)
    for i in range(8):
        out = pl.ds(i * 256, 256)
        gs[:, out] = dot(own[2], weight_rows(1, 0, i), NT) + dot(own[3], weight_rows(1, 1, i), NT)
    wait_bytes(rs2.at[pl.ds(0, NZ - 1)], rs_sem.at[3])
    for t in range(1, NZ):
        gw_ref[...] += rs2[(z + t) % NZ].astype(F32)
    exchanged(0)
    for i in range(8):
        out = pl.ds(i * 256, 256)
        gs[:, out] += dot(own[0], weight_rows(0, 0, i), NT)
    own_rows.wait()
    bk[1].collect(keep(pk.at[1]))
    exchange(1)
    exchanged(1)

    def stores(i):
        at = pl.ds(i * 64, 64)
        return pltpu.make_async_copy(rows.at[pl.ds(quarter + i * 64, 64)], gs_out.at[at], out_sem.at[2 + i])

    for i in range(8):
        out = pl.ds(i * 256, 256)
        gs[:, out] += dot(own[1], weight_rows(0, 1, i), NT)
    for i in range(quarter // 64):

        @pl.loop(0, 2)
        def _(t):
            at = pl.ds(i * 64 + t * 32, 32)
            raw = rows[at].astype(F32)
            inverse = row_scale(raw)
            unit = raw * inverse
            grad_unit = gs[at] * gain[...]
            slope = inverse * (grad_unit - unit * jnp.mean(grad_unit * unit, axis=-1, keepdims=True))
            rows[pl.ds(quarter + i * 64 + t * 32, 32)] = slope.astype(BF16)

        stores(i).start()

    for trip in (ek, ev, bv, *bk):
        trip.finish()
    for n in range(2):
        for away in range(1, NTP):
            weight_move(n, away).wait_send()
            weight_pass(n, away).wait_send()
    wait_bytes(asked.at[pl.ds(0, NZ - 1), 0], ask_sem.at[0])
    wait_bytes(asked.at[pl.ds(0, NJ - 1)], ask_sem.at[2])
    wait_bytes(rs1.at[pl.ds(0, NJ - 1)], rs_sem.at[0])
    wait_bytes(rs2.at[pl.ds(0, NZ - 1)], rs_sem.at[2])
    dq_store.wait()
    for i in range(quarter // 64):
        stores(i).wait()


def local(queries, gate_pre, cotangent, store, store_gain, w_key, w_value, owners, slots):
    tokens, width = queries.shape
    rows, features = store.shape
    heads = width // HD
    blocks = tokens // 128
    quarter = rows // NTP
    vmem = pl.BlockSpec(memory_space=pltpu.VMEM)
    smem = pl.BlockSpec(memory_space=pltpu.SMEM)
    far = pl.BlockSpec(memory_space=pltpu.HBM)
    piece = (PLEN, width)
    slim = (PLEN, HD)
    dma = pltpu.SemaphoreType.DMA
    grad_queries, grad_store, grad_w_value = pl.pallas_call(
        kernel,
        out_shape=(
            jax.ShapeDtypeStruct((tokens, width), BF16),
            jax.ShapeDtypeStruct((quarter, features), BF16),
            jax.ShapeDtypeStruct((features // NST, width), F32),
        ),
        in_specs=[smem, smem] + [far] * 6 + [vmem],
        out_specs=(far, far, vmem),
        scratch_shapes=[
            pltpu.VMEM((rows, features), BF16),
            pltpu.VMEM((2, PASSAGES) + piece, BF16),
            pltpu.VMEM((NZ, NJ, 1, 128), jnp.int32),
            pltpu.VMEM((META_ROWS, 128), jnp.int32),
            pltpu.SMEM((META_ROWS, 128), jnp.int32),
            pltpu.VMEM((tokens, width), BF16),
            pltpu.VMEM((tokens, width), BF16),
            pltpu.VMEM((2, PASSAGES) + piece, BF16),
            pltpu.VMEM((2, PASSAGES) + piece, BF16),
            pltpu.VMEM((PASSAGES,) + piece, BF16),
            pltpu.VMEM((PASSAGES,) + piece, BF16),
            pltpu.VMEM((2, 4, NJ) + piece, BF16),
            pltpu.VMEM((2, 2, NJ) + piece, BF16),
            pltpu.VMEM((2, NST) + piece, BF16),
            pltpu.VMEM((2, 2 * NZ) + piece, BF16),
            pltpu.VMEM((NST,) + piece, BF16),
            pltpu.VMEM((NST,) + piece, BF16),
            pltpu.VMEM((NST,) + piece, BF16),
            pltpu.VMEM((NST,) + piece, BF16),
            pltpu.VMEM((2 * NZ,) + piece, BF16),
            pltpu.VMEM((6, NJ) + piece, BF16),
            pltpu.VMEM((3, PASSAGES) + piece, BF16),
            pltpu.VMEM((3, PASSAGES) + piece, BF16),
            pltpu.VMEM((2, NST) + slim, BF16),
            pltpu.VMEM((2, NST) + slim, BF16),
            pltpu.VMEM((2, 2 * NZ) + slim, BF16),
            pltpu.VMEM((2, 6, NJ) + slim, BF16),
            pltpu.VMEM((2, 3, PASSAGES) + slim, BF16),
            pltpu.VMEM((2, 3, PASSAGES) + slim, BF16),
            pltpu.VMEM((blocks, heads, 256, 128), BF16),
            pltpu.VMEM((blocks * 4,) + piece, BF16),
            pltpu.VMEM((BASE + PASSAGES,) + slim, F32),
            pltpu.VMEM((rows, width), BF16),
            pltpu.VMEM((2, rows, HD), BF16),
            pltpu.VMEM((2, 2, NST // 2, PLEN, HD * NTP), BF16),
            pltpu.VMEM((4, quarter, HD * NTP), BF16),
            pltpu.VMEM((NZ, NJ, features // NST, width), BF16),
            pltpu.VMEM((NJ, NZ, features // NST, width), BF16),
            pltpu.VMEM((NZ, features // NST, width), BF16),
            pltpu.VMEM((NZ, features // NST, width), BF16),
            pltpu.VMEM((quarter, features), F32),
            dma((2, 2)),
            dma((2, 12)),
            dma((2,)),
            dma((2, 1)),
            dma((2,)),
            dma((2, 2 * NZ)),
            dma((3, 2)),
            dma((3, 9)),
            dma((3,)),
            dma((3, NZ)),
            dma((3,)),
            dma((3, 2 * NZ)),
            dma((rows // 256,)),
            dma((5,)),
            dma((9,)),
            dma((2, 4, NTP)),
            dma((4, 2, NTP)),
            dma((4,)),
            dma((2 + quarter // 64,)),
        ],
        cost_estimate=pl.CostEstimate(flops=10**10, bytes_accessed=10**7, transcendentals=0),
        compiler_params=pltpu.CompilerParams(collective_id=0, has_side_effects=True, vmem_limit_bytes=67043328),
        name="passages",
    )(owners.T, slots.T, queries, gate_pre, cotangent, store, *(w.reshape(-1, PLEN, width) for w in (w_key, w_value)), store_gain[None])
    return (grad_queries.astype(F32), grad_store.astype(F32), grad_w_value)


def solution(mesh):
    placed = (
        P("st", "tp"),
        P("st", "tp"),
        P("st", "tp"),
        P("st", None),
        P(),
        P(None, "tp"),
        P(None, "tp"),
        P("st", None),
        P("st", None),
    )
    return jax.shard_map(
        local,
        mesh=mesh,
        in_specs=placed,
        out_specs=(P("st", "tp"), P(("st", "tp"), None), P("st", "tp")),
        check_vma=False,
    )
```

```python
import functools

import jax
import jax.numpy as jnp
from jax import lax
from jax.experimental import pallas as pl
from jax.experimental.pallas import tpu as pltpu
from jax.sharding import PartitionSpec as P

HD = 128
PLEN = 64
EPS = 1e-06
NZ = 8
NJ = 8
NST = NZ * NJ
NTP = 4
MESH = pl.DeviceIdType.MESH
NT = (((1,), (1,)), ((), ()))
TN = (((0,), (0,)), ((), ()))
F32 = jnp.float32
BF16 = jnp.bfloat16


def dot(left, right, dims=(((1,), (0,)), ((), ()))):
    return lax.dot_general(left, right, dims, preferred_element_type=F32)


def row_scale(rows):
    return lax.rsqrt(jnp.mean(rows * rows, axis=-1, keepdims=True) + EPS)


def remote(src, dst, send_sem, recv_sem, axis, peer):
    return pltpu.make_async_remote_copy(
        src_ref=src, dst_ref=dst, send_sem=send_sem, recv_sem=recv_sem, device_id={axis: peer}, device_id_type=MESH
    )


def wait_bytes(ref, sem):
    pltpu.make_async_copy(ref, ref, sem).wait()


def greet(me, tp):
    z, j = me // NJ, me % NJ
    barrier = pltpu.get_barrier_semaphore()
    for t in range(1, NJ):
        pl.semaphore_signal(barrier, inc=1, device_id={"st": z * NJ + (j + t) % NJ}, device_id_type=MESH)
    for t in range(1, NZ):
        pl.semaphore_signal(barrier, inc=1, device_id={"st": (z + t) % NZ * NJ + j}, device_id_type=MESH)
    if tp is not None:
        for t in range(1, NTP):
            pl.semaphore_signal(barrier, inc=1, device_id={"tp": (tp + t) % NTP}, device_id_type=MESH)
    return barrier, NJ + NZ - 2 + (0 if tp is None else NTP - 1)


NY = NJ // 2


PASSAGES = 20
PART = PASSAGES // 2
BASE = 24
PREV, LAST, PLACE, NAMED, META_ROWS = 64, 68, 72, 73, 80


class Column:
    def __init__(self, me, z_send, z_recv, y_send, y_recv):
        self.z, self.j, self.long = me // NJ, me % NJ, 1 - 2 * (me % 2)
        self.z_send, self.z_recv, self.y_send, self.y_recv = z_send, z_recv, y_send, y_recv

    def plane(self, steps):
        return (self.z + steps * self.long + NZ) % NZ

    def step(self, side, number, src, dst):
        peer = self.plane(1 - 2 * side) * NJ + self.j
        return remote(src, dst, self.z_send.at[side], self.z_recv.at[number], "st", peer)

    def beside(self, steps, core):
        return (self.j // 2 + steps + NY) % NY * 2 + core

    def spread(self, src, dst, plane, recv_sem):
        z, j, core = self.z, self.j, self.j % 2
        pltpu.make_async_copy(src.at[plane * NJ + j], dst.at[plane * NJ + j], recv_sem).start()
        for steps, to in ((2, 0), (2, 1), (1, 0), (-1, 0), (1, 1), (-1, 1), (0, 1 - core)):
            other = self.beside(steps, to)
            remote(src.at[plane * NJ + other], dst.at[plane * NJ + j], self.y_send, recv_sem, "st", z * NJ + other).start()


class Outward(Column):
    def __init__(self, me, meta, table, near, far, picked, passed, column, fin, *sems):
        super().__init__(me, *sems)
        self.meta, self.table, self.near, self.far = meta, table, near, far
        self.picked, self.passed, self.column, self.fin = picked, passed, column, fin

    def launch(self, part, side):
        at = pl.ds(part * PART, PART)
        return self.step(side, 2 * side + part, self.table.at[at], self.near.at[side, at])

    def relay(self, part):
        at = pl.ds(part * PART, PART)
        return self.step(0, 4 + part, self.near.at[0, at], self.far.at[at])

    def hop(self, name):
        column, picked, passed, at = self.column, self.picked, self.passed, self.block
        return {
            "s2": lambda: self.step(1, 6, picked.at[0], column.at[at(self.plane(1))]),
            "s3": lambda: self.step(1, 7, picked.at[1], passed.at[1]),
            "s3b": lambda: self.step(1, 8, passed.at[1], column.at[at(self.plane(2))]),
            "l3": lambda: self.step(0, 9, picked.at[2], column.at[at(self.plane(-2))]),
            "l4": lambda: self.step(0, 10, picked.at[3], passed.at[0]),
            "l4b": lambda: self.step(0, 11, passed.at[0], column.at[at(self.plane(-3))]),
        }[name]()

    def block(self, plane):
        return pl.ds(plane * NJ, NJ)

    def pick(self, table, owner_plane, reader_plane, out, first):
        meta, owner = self.meta, owner_plane * NJ + self.j

        @pl.loop(0, NJ)
        def _(t):
            out[first + t] = table[jnp.maximum(meta[reader_plane * NJ + t, owner], 0)]

    def deliver(self, plane):
        self.spread(self.column, self.fin, plane, self.y_recv.at[0])

    def start(self, part):
        for side in range(2):
            self.launch(part, side).start()

    def own(self):
        self.pick(self.table, self.z, self.z, self.column, self.z * NJ)
        self.deliver(self.z)

    def forward(self, part):
        self.launch(part, 0).wait_recv()
        self.relay(part).start()

    def first(self):
        for part in range(2):
            self.launch(part, 1).wait_recv()
        owner = self.plane(1)
        self.pick(self.near.at[1], owner, self.plane(-2), self.picked.at[1], 0)
        self.hop("s3").start()
        self.pick(self.near.at[1], owner, self.plane(-1), self.picked.at[0], 0)
        self.hop("s2").start()
        for owner, side in ((self.plane(-1), 0), (self.plane(1), 1)):
            self.pick(self.near.at[side], owner, self.z, self.column, owner * NJ)
            self.deliver(owner)

    def second(self):
        self.hop("s3").wait_recv()
        self.hop("s3b").start()
        for part in range(2):
            self.relay(part).wait_recv()
        owner = self.plane(-2)
        self.pick(self.far, owner, self.plane(2), self.picked.at[3], 0)
        self.hop("l4").start()
        self.pick(self.far, owner, self.plane(1), self.picked.at[2], 0)
        self.hop("l3").start()
        self.pick(self.far, owner, self.z, self.column, owner * NJ)
        self.deliver(owner)
        self.hop("s2").wait_recv()
        self.deliver(self.plane(2))

    def third(self):
        self.hop("l4").wait_recv()
        self.hop("l4b").start()
        self.hop("s3b").wait_recv()
        self.deliver(self.plane(3))
        self.hop("l3").wait_recv()
        self.deliver(self.plane(-3))

    def fourth(self):
        self.hop("l4b").wait_recv()
        self.deliver(self.plane(-4))

    def arrive(self):
        wait_bytes(self.fin, self.y_recv.at[0])

    def finish(self):
        wait_bytes(self.column, self.z_send.at[0])
        wait_bytes(self.column.at[pl.ds(0, 44)], self.z_send.at[1])
        wait_bytes(self.column.at[pl.ds(0, NZ * (NJ - 1))], self.y_send)


class Homeward(Column):
    def __init__(self, me, meta, x, column, slots, sums, gained, stage, *sems):
        super().__init__(me, *sems)
        self.meta, self.x, self.column, self.slots = meta, x, column, slots
        self.sums, self.gained, self.stage = sums, gained, stage

    def block(self, plane):
        return pl.ds(plane * NJ, NJ)

    def hop(self, name):
        mine = lambda steps: self.column.at[self.block(self.plane(steps))]
        slots, sums, gained = self.slots, self.sums, self.gained
        return {
            "l4": lambda: self.step(1, 0, mine(-4), slots.at[0]),
            "l3": lambda: self.step(1, 1, mine(-3), slots.at[1]),
            "l4b": lambda: self.step(1, 2, slots.at[0], slots.at[2]),
            "l2": lambda: self.step(1, 3, sums.at[0], gained.at[0]),
            "l1": lambda: self.step(1, 4, sums.at[1], gained.at[1]),
            "s3": lambda: self.step(0, 5, mine(3), slots.at[3]),
            "s2": lambda: self.step(0, 6, mine(2), slots.at[4]),
            "s3b": lambda: self.step(0, 7, slots.at[3], slots.at[5]),
            "s1": lambda: self.step(0, 8, sums.at[2], gained.at[2]),
        }[name]()

    def start(self, *steps):
        for one in steps:
            plane = self.plane(one)
            self.spread(self.x, self.column, plane, self.y_recv.at[plane])

    def gathered(self, steps):
        plane = self.plane(steps)
        wait_bytes(self.column.at[self.block(plane)], self.y_recv.at[plane])

    def add_up(self, combo, planes, slots, bases, store):
        meta, stage = self.meta, self.stage
        width = self.x.shape[-1]
        for first in range(0, width, HD):
            cols = pl.ds(first, HD)

            @pl.loop(0, PASSAGES)
            def _(p):
                total = jnp.zeros(stage.shape[1:], F32)
                for base in bases:
                    total = total + base[p, :, cols].astype(F32)
                stage[BASE + p] = total

            for rank, (plane, (ref, start)) in enumerate(zip(planes, slots)):

                @pl.loop(0, NJ)
                def _(t):
                    stage[rank * NJ + t] = ref[start + t, :, cols].astype(F32) + stage[meta[PREV + combo, plane * NJ + t]]

            @pl.loop(0, PASSAGES)
            def _(p):
                store(p, cols, stage[meta[LAST + combo, p]].astype(BF16))

    def into(self, number):
        def store(p, cols, value):
            self.sums[number, p, :, cols] = value

        return store

    def first(self):
        self.gathered(-4)
        self.hop("l4").start()
        self.gathered(3)
        self.hop("s3").start()
        self.gathered(-3)
        self.hop("l3").start()
        self.gathered(2)
        self.hop("s2").start()

    def second(self):
        self.hop("l4").wait_recv()
        self.hop("l4b").start()
        self.hop("s3").wait_recv()
        self.hop("s3b").start()

    def third(self):
        self.gathered(-2)
        self.hop("l3").wait_recv()
        self.hop("l4b").wait_recv()
        planes = (self.plane(2), self.plane(1), self.z)
        slots = ((self.slots.at[2], 0), (self.slots.at[1], 0), (self.column, self.plane(-2) * NJ))
        self.add_up(0, planes, slots, (), self.into(0))
        self.hop("l2").start()
        self.gathered(1)
        self.hop("s2").wait_recv()
        self.hop("s3b").wait_recv()
        planes = (self.plane(-2), self.plane(-1), self.z)
        slots = ((self.slots.at[5], 0), (self.slots.at[4], 0), (self.column, self.plane(1) * NJ))
        self.add_up(2, planes, slots, (), self.into(2))
        self.hop("s1").start()

    def fourth(self):
        self.gathered(-1)
        self.hop("l2").wait_recv()
        slots = ((self.column, self.plane(-1) * NJ),)
        self.add_up(1, (self.z,), slots, (self.gained.at[0],), self.into(1))
        self.hop("l1").start()

    def collect(self, store):
        self.gathered(0)
        self.hop("l1").wait_recv()
        self.hop("s1").wait_recv()
        slots = ((self.column, self.z * NJ),)
        self.add_up(3, (self.z,), slots, (self.gained.at[1], self.gained.at[2]), store)

    def finish(self):
        wait_bytes(self.column, self.z_send.at[1])
        wait_bytes(self.column.at[pl.ds(0, 44)], self.z_send.at[0])
        wait_bytes(self.column.at[pl.ds(0, NZ * (NJ - 1))], self.y_send)


def plans(asked, me, place, named, meta):
    z, j, long = me // NJ, me % NJ, 1 - 2 * (me % 2)
    everyone = asked[...].reshape(NST, 128)
    meta[0:NST] = everyone
    lanes = lax.broadcasted_iota(jnp.int32, (NST, 128), 1)
    reader = lax.broadcasted_iota(jnp.int32, (NST, 128), 0)
    combos = ((-2, 2, 3, -1), (-1, 0, 1, -1), (1, -2, 3, 1), (0, 0, 1, 1))
    for number, (owner, start, count, way) in enumerate(combos):
        owner = (z + owner * long + NZ) % NZ * NJ + j
        start = (z + start * long + NZ) % NZ

        def rank(index):
            return ((index // NJ - start) * (way * long) + 2 * NZ) % NZ * NJ + index % NJ

        mine, other = rank(reader), rank(lanes)
        column = jnp.max(jnp.where(lanes == owner, everyone, -1), axis=1, keepdims=True)
        across = jnp.max(jnp.where(lanes == reader, column, -1), axis=0, keepdims=True)
        inside = mine < count * NJ
        before = jnp.max(jnp.where(inside & (mine < other) & (column == across), mine, -1), axis=0, keepdims=True)
        last = jnp.max(jnp.where(inside & (column == lanes), mine, -1), axis=0, keepdims=True)
        spot = lax.broadcasted_iota(jnp.int32, (1, 128), 1)
        meta[PREV + number : PREV + number + 1] = jnp.where(before < 0, BASE + jnp.maximum(across, 0), before)
        meta[LAST + number : LAST + number + 1] = jnp.where(last < 0, BASE + spot, last)
    meta[PLACE : PLACE + 1] = place
    meta[NAMED : NAMED + 1] = named
    meta[NAMED + 1 : META_ROWS] = jnp.zeros((META_ROWS - NAMED - 1, 128), jnp.int32)


def kernel(
    owners, slots, q_in, gate_in, cot_in, store_in, wk_in, wv_in, gain,
    dq_out, gs_out, gw_ref,
    rows, tables, asked, plan, meta, q, g, near_k, near_v, far_k, far_v, picked, passed, out_column, fin_k, fin_v, x, column, slot_v, sum_v, gain_v,
    xk, columnk, slot_k, sum_k, gain_k, weights, terms, stage, pv, pk, wide_w, own, gwb, rs1, rsb, rs2, gs,
    oz_send, oz_recv, oy_send, oy_recv, hz_send, hz_recv, hy_send, hy_recv,
    row_sem, ask_sem, in_sem, tp_sem, w_sem, rs_sem, out_sem,
):
    me = lax.axis_index("st")
    tp = lax.axis_index("tp")
    z, j = me // NJ, me % NJ
    core = me % 2
    scale = HD ** (-0.5)
    heads = q.shape[1] // HD
    width = q.shape[1]
    blocks = weights.shape[0]
    quarter = gs.shape[0]
    barrier, peers = greet(me, tp)
    slim = pl.ds(pl.multiple_of(tp * HD, HD), HD)

    def out_sems(n):
        return oz_send.at[n], oz_recv.at[n], oy_send.at[n], oy_recv.at[n]

    def home_sems(n):
        return hz_send.at[n], hz_recv.at[n], hy_send.at[n], hy_recv.at[n]

    fins = (fin_k, fin_v)
    ek, ev = (
        Outward(me, meta, tables.at[n], (near_k, near_v)[n], (far_k, far_v)[n], picked.at[n], passed.at[n], out_column.at[n], fins[n], *out_sems(n))
        for n in range(2)
    )
    bv = Homeward(me, meta, x, column, slot_v, sum_v, gain_v, stage, *home_sems(0))
    bk = [
        Homeward(me, meta, xk.at[h], columnk.at[h], slot_k.at[h], sum_k.at[h], gain_k.at[h], stage, *home_sems(1 + h))
        for h in range(2)
    ]

    weight_loads = [
        pltpu.make_async_copy(ref.at[:, :, pl.ds(h * HD, HD)], wide_w.at[n, h, :, :, slim], in_sem.at[2 * n + h])
        for n, ref in enumerate((wk_in, wv_in))
        for h in range(2)
    ]
    first_loads = [
        pltpu.make_async_copy(ref, x.at[pl.ds(n * NST // 2, NST // 2)], in_sem.at[7 + n])
        for n, ref in enumerate((wk_in, wv_in))
    ]
    token_loads = [
        pltpu.make_async_copy(q_in, q, in_sem.at[4]),
        pltpu.make_async_copy(cot_in, g, in_sem.at[5]),
        pltpu.make_async_copy(gate_in, pv.at[pl.ds(0, gate_in.shape[0])], in_sem.at[6]),
    ]
    count = rows.shape[0] // 256

    def chunk(i):
        return pl.ds(i * 256, 256)

    def row_load(i):
        return pltpu.make_async_copy(store_in.at[chunk(i)], rows.at[chunk(i)], row_sem.at[i])

    row_load(0).start()
    for load in first_loads:
        load.start()
    for i in range(1, count):
        row_load(i).start()
    for load in weight_loads + token_loads:
        load.start()

    lane = lax.broadcasted_iota(jnp.int32, (1, 128), 1)
    request = jnp.full((1, 128), -1, jnp.int32)
    place = jnp.zeros((1, 128), jnp.int32)
    named = jnp.zeros((1, 128), jnp.int32)
    per_block = owners.shape[0]
    for b in range(blocks):
        for i in range(per_block):
            at = b * per_block + i
            owner, slot = owners[i, b], slots[i, b]
            request = jnp.where(lane == owner, slot, request)
            place = jnp.where(lane == owner, at, place)
            named = jnp.where(lane == at, owner, named)
    asked[z, j] = request
    for load in first_loads:
        load.wait()

    def project(i):
        at = chunk(i)
        row_load(i).wait()

        @pl.loop(0, 8)
        def _(t):
            tile = pl.ds(i * 256 + t * 32, 32)
            raw = rows[tile].astype(F32)
            rows[tile] = (raw * row_scale(raw) * gain[...]).astype(BF16)

        for n in range(2):
            weight = x[pl.ds(n * NST // 2, NST // 2)].reshape(rows.shape[1], width)
            tables[n, pl.ds(4 * i, 4)] = dot(rows[at], weight).astype(BF16).reshape(4, PLEN, width)

    project(0)
    project(1)
    project(2)
    pl.semaphore_wait(barrier, peers)
    for t in range(1, NZ):
        other = (z + t) % NZ
        remote(asked.at[z, j], asked.at[z, j], ask_sem.at[0], ask_sem.at[1], "st", other * NJ + j).start()
    ek.start(0)
    project(3)
    project(4)
    ek.start(1)
    wait_bytes(asked.at[pl.ds(0, NZ - 1), 0], ask_sem.at[1])
    for t in range(1, NJ):
        remote(asked.at[:, j], asked.at[:, j], ask_sem.at[2], ask_sem.at[3], "st", z * NJ + (j + t) % NJ).start()
    ek.forward(0)
    ev.start(0)
    ek.forward(1)
    ev.start(1)

    part = wide_w.shape[2] // 2
    half_rows = pl.ds(core * part, part)

    def weight_move(n, away):
        ref = wide_w.at[n, :, half_rows, :, slim]
        return remote(ref, ref, w_sem.at[0, n, away], w_sem.at[1, n, away], "tp", (tp + away) % NTP)

    def weight_pass(n, away):
        ref = wide_w.at[n, :, half_rows, :, pl.ds(pl.multiple_of((tp + NTP - away) % NTP * HD, HD), HD)]
        return remote(ref, ref, w_sem.at[2, n, away], w_sem.at[3, n, away], "st", me + 1 - 2 * core)

    for load in weight_loads:
        load.wait()
    for n in range(2):
        for away in range(1, NTP):
            weight_move(n, away).start()
    wait_bytes(asked.at[pl.ds(0, NJ - 1)], ask_sem.at[3])
    plans(asked, me, place, named, plan)
    sent_plan = pltpu.make_async_copy(plan, meta, ask_sem.at[4])
    sent_plan.start()
    for load in token_loads:
        load.wait()

    @pl.loop(0, blocks)
    def _(b):
        at = pl.ds(b * 128, 128)
        g[at] = (jax.nn.sigmoid(pv[at].astype(F32)) * g[at].astype(F32)).astype(BF16)

    sent_plan.wait()
    ek.first()
    ek.own()
    ek.second()
    ek.third()
    ev.forward(0)
    ev.forward(1)
    ev.first()
    ek.fourth()
    ev.own()
    ek.arrive()

    def joined(n, b, cols):
        return jnp.concatenate([fins[n][meta[NAMED, b * 4 + i], :, cols] for i in range(4)], axis=0)

    def weigh(b):
        at = pl.ds(b * 128, 128)
        for h in range(heads):
            cols = pl.ds(h * HD, HD)
            score = dot(joined(0, b, cols), q[at, cols], NT) * scale
            raised = jnp.exp(score - jnp.max(score, axis=0, keepdims=True))
            weight = raised / jnp.sum(raised, axis=0, keepdims=True)
            weight = weight.astype(BF16)
            weights[b, h] = weight
            terms[pl.ds(b * 4, 4), :, cols] = dot(weight, g[at, cols]).astype(BF16).reshape(4, PLEN, HD)

    pl.loop(0, blocks // 4)(weigh)
    ev.second()
    pl.loop(blocks // 4, blocks)(weigh)

    @pl.loop(0, NST)
    def _(o):
        x[o] = terms[meta[PLACE, o]]

    bv.start(-4, 3, -3, 2, -2)
    ev.third()
    ev.fourth()
    bv.first()
    bv.start(1, -1, 0)
    for n in range(2):
        for away in range(1, NTP):
            weight_move(n, away).wait_recv()
            weight_pass(n, away).start()
    bv.second()
    ev.arrive()

    @pl.loop(0, blocks)
    def _(b):
        at = pl.ds(b * 128, 128)
        for h in range(heads):
            cols = pl.ds(h * HD, HD)
            steep = dot(joined(1, b, cols), g[at, cols], NT)
            weight = weights[b, h].astype(F32)
            delta = jnp.sum(weight * steep, axis=0, keepdims=True)
            slope = (weight * (steep - delta)).astype(BF16)
            terms[pl.ds(b * 4, 4), :, cols] = (dot(slope, q[at, cols]) * scale).astype(BF16).reshape(4, PLEN, HD)
            q[at, cols] = (dot(slope, joined(0, b, cols), TN) * scale).astype(BF16)

    dq_store = pltpu.make_async_copy(q, dq_out, out_sem.at[0])
    dq_store.start()

    @pl.loop(0, NST)
    def _(o):
        for h in range(2):
            xk[h, o] = terms[meta[PLACE, o], :, pl.ds(h * HD, HD)]

    bk[0].start(-4, 3, -3, 2, -2)
    bv.third()
    bk[0].first()
    bk[0].start(1, -1, 0)
    bk[1].start(-4, 3, -3, 2, -2)
    bv.fourth()
    bk[0].second()
    bk[1].first()
    bk[1].start(1, -1, 0)

    def keep(ref):
        def store(p, cols, value):
            ref[pl.ds(pl.multiple_of(p * PLEN, PLEN), PLEN), cols] = value

        return store

    bv.collect(keep(pv))

    def across(n, away):
        src = (pk.at[0], pk.at[1], pv.at[:, pl.ds(0, HD)], pv.at[:, pl.ds(HD, HD)])[n]
        peer = (tp + away) % NTP
        at = pl.ds(pl.multiple_of(peer * quarter, 16), quarter)
        return remote(src.at[at], own.at[n, :, slim], tp_sem.at[0, n, away], tp_sem.at[1, n, away], "tp", peer)

    def kept(n):
        src = (pk.at[0], pk.at[1], pv.at[:, pl.ds(0, HD)], pv.at[:, pl.ds(HD, HD)])[n]
        return pltpu.make_async_copy(src.at[pl.ds(pl.multiple_of(tp * quarter, 16), quarter)], own.at[n, :, slim], tp_sem.at[0, n, 0])

    def exchange(n):
        kept(n).start()
        for away in range(1, NTP):
            across(n, away).start()

    def exchanged(n):
        kept(n).wait()
        for away in range(1, NTP):
            across(n, away).wait()

    def weight_rows(n, h, i):
        return wide_w[n, h, 4 * i : 4 * i + 4].reshape(256, HD * NTP)

    exchange(2)
    exchange(3)
    bk[0].third()
    bk[1].second()
    for i in range(NZ):
        gwb[i] = dot(rows[:, i * 256 : (i + 1) * 256], pv[...], TN).astype(BF16).reshape(NJ, 32, width)
    own_rows = pltpu.make_async_copy(
        store_in.at[pl.ds(pl.multiple_of(tp * quarter, 16), quarter)], rows.at[pl.ds(0, quarter)], out_sem.at[1]
    )
    own_rows.start()
    for t in range(1, NJ):
        other = (j + t) % NJ
        remote(gwb.at[:, other], rs1.at[j], rs_sem.at[0], rs_sem.at[1], "st", z * NJ + other).start()
    bk[0].fourth()
    bk[1].third()
    wait_bytes(rs1.at[pl.ds(0, NJ - 1)], rs_sem.at[1])
    total = gwb[:, j].astype(F32)
    for t in range(1, NJ):
        total = total + rs1[(j + t) % NJ].astype(F32)
    rsb[...] = total.astype(BF16)
    gw_ref[...] = gwb[z, j].astype(F32)
    for t in range(1, NJ):
        gw_ref[...] += rs1[(j + t) % NJ, z].astype(F32)
    for t in range(1, NZ):
        other = (z + t) % NZ
        remote(rsb.at[other], rs2.at[z], rs_sem.at[2], rs_sem.at[3], "st", other * NJ + j).start()
    bk[0].collect(keep(pk.at[0]))
    exchange(0)
    bk[1].fourth()
    for n in range(2):
        for away in range(1, NTP):
            weight_pass(n, away).wait_recv()
    exchanged(2)
    exchanged(3)
    for i in range(8):
        out = pl.ds(i * 256, 256)
        gs[:, out] = dot(own[2], weight_rows(1, 0, i), NT) + dot(own[3], weight_rows(1, 1, i), NT)
    wait_bytes(rs2.at[pl.ds(0, NZ - 1)], rs_sem.at[3])
    for t in range(1, NZ):
        gw_ref[...] += rs2[(z + t) % NZ].astype(F32)
    exchanged(0)
    for i in range(8):
        out = pl.ds(i * 256, 256)
        gs[:, out] += dot(own[0], weight_rows(0, 0, i), NT)
    own_rows.wait()
    bk[1].collect(keep(pk.at[1]))
    exchange(1)
    exchanged(1)

    def stores(i):
        at = pl.ds(i * 64, 64)
        return pltpu.make_async_copy(rows.at[pl.ds(quarter + i * 64, 64)], gs_out.at[at], out_sem.at[2 + i])

    for i in range(8):
        out = pl.ds(i * 256, 256)
        gs[:, out] += dot(own[1], weight_rows(0, 1, i), NT)
    for i in range(quarter // 64):

        @pl.loop(0, 2)
        def _(t):
            at = pl.ds(i * 64 + t * 32, 32)
            raw = rows[at].astype(F32)
            inverse = row_scale(raw)
            unit = raw * inverse
            grad_unit = gs[at] * gain[...]
            slope = inverse * (grad_unit - unit * jnp.mean(grad_unit * unit, axis=-1, keepdims=True))
            rows[pl.ds(quarter + i * 64 + t * 32, 32)] = slope.astype(BF16)

        stores(i).start()

    for trip in (ek, ev, bv, *bk):
        trip.finish()
    for n in range(2):
        for away in range(1, NTP):
            weight_move(n, away).wait_send()
            weight_pass(n, away).wait_send()
    wait_bytes(asked.at[pl.ds(0, NZ - 1), 0], ask_sem.at[0])
    wait_bytes(asked.at[pl.ds(0, NJ - 1)], ask_sem.at[2])
    wait_bytes(rs1.at[pl.ds(0, NJ - 1)], rs_sem.at[0])
    wait_bytes(rs2.at[pl.ds(0, NZ - 1)], rs_sem.at[2])
    dq_store.wait()
    for i in range(quarter // 64):
        stores(i).wait()


def local(queries, gate_pre, cotangent, store, store_gain, w_key, w_value, owners, slots):
    tokens, width = queries.shape
    rows, features = store.shape
    heads = width // HD
    blocks = tokens // 128
    quarter = rows // NTP
    vmem = pl.BlockSpec(memory_space=pltpu.VMEM)
    smem = pl.BlockSpec(memory_space=pltpu.SMEM)
    far = pl.BlockSpec(memory_space=pltpu.HBM)
    piece = (PLEN, width)
    slim = (PLEN, HD)
    dma = pltpu.SemaphoreType.DMA
    grad_queries, grad_store, grad_w_value = pl.pallas_call(
        kernel,
        out_shape=(
            jax.ShapeDtypeStruct((tokens, width), BF16),
            jax.ShapeDtypeStruct((quarter, features), BF16),
            jax.ShapeDtypeStruct((features // NST, width), F32),
        ),
        in_specs=[smem, smem] + [far] * 6 + [vmem],
        out_specs=(far, far, vmem),
        scratch_shapes=[
            pltpu.VMEM((rows, features), BF16),
            pltpu.VMEM((2, PASSAGES) + piece, BF16),
            pltpu.VMEM((NZ, NJ, 1, 128), jnp.int32),
            pltpu.VMEM((META_ROWS, 128), jnp.int32),
            pltpu.SMEM((META_ROWS, 128), jnp.int32),
            pltpu.VMEM((tokens, width), BF16),
            pltpu.VMEM((tokens, width), BF16),
            pltpu.VMEM((2, PASSAGES) + piece, BF16),
            pltpu.VMEM((2, PASSAGES) + piece, BF16),
            pltpu.VMEM((PASSAGES,) + piece, BF16),
            pltpu.VMEM((PASSAGES,) + piece, BF16),
            pltpu.VMEM((2, 4, NJ) + piece, BF16),
            pltpu.VMEM((2, 2, NJ) + piece, BF16),
            pltpu.VMEM((2, NST) + piece, BF16),
            pltpu.VMEM((NST,) + piece, BF16),
            pltpu.VMEM((NST,) + piece, BF16),
            pltpu.VMEM((NST,) + piece, BF16),
            pltpu.VMEM((NST,) + piece, BF16),
            pltpu.VMEM((6, NJ) + piece, BF16),
            pltpu.VMEM((3, PASSAGES) + piece, BF16),
            pltpu.VMEM((3, PASSAGES) + piece, BF16),
            pltpu.VMEM((2, NST) + slim, BF16),
            pltpu.VMEM((2, NST) + slim, BF16),
            pltpu.VMEM((2, 6, NJ) + slim, BF16),
            pltpu.VMEM((2, 3, PASSAGES) + slim, BF16),
            pltpu.VMEM((2, 3, PASSAGES) + slim, BF16),
            pltpu.VMEM((blocks, heads, 256, 128), BF16),
            pltpu.VMEM((blocks * 4,) + piece, BF16),
            pltpu.VMEM((BASE + PASSAGES,) + slim, F32),
            pltpu.VMEM((rows, width), BF16),
            pltpu.VMEM((2, rows, HD), BF16),
            pltpu.VMEM((2, 2, NST // 2, PLEN, HD * NTP), BF16),
            pltpu.VMEM((4, quarter, HD * NTP), BF16),
            pltpu.VMEM((NZ, NJ, features // NST, width), BF16),
            pltpu.VMEM((NJ, NZ, features // NST, width), BF16),
            pltpu.VMEM((NZ, features // NST, width), BF16),
            pltpu.VMEM((NZ, features // NST, width), BF16),
            pltpu.VMEM((quarter, features), F32),
            dma((2, 2)),
            dma((2, 12)),
            dma((2,)),
            dma((2, 1)),
            dma((3, 2)),
            dma((3, 9)),
            dma((3,)),
            dma((3, NZ)),
            dma((rows // 256,)),
            dma((5,)),
            dma((9,)),
            dma((2, 4, NTP)),
            dma((4, 2, NTP)),
            dma((4,)),
            dma((2 + quarter // 64,)),
        ],
        cost_estimate=pl.CostEstimate(flops=10**10, bytes_accessed=10**7, transcendentals=0),
        compiler_params=pltpu.CompilerParams(collective_id=0, has_side_effects=True, vmem_limit_bytes=67043328),
        name="passages",
    )(owners.T, slots.T, queries, gate_pre, cotangent, store, *(w.reshape(-1, PLEN, width) for w in (w_key, w_value)), store_gain[None])
    return (grad_queries.astype(F32), grad_store.astype(F32), grad_w_value)


def solution(mesh):
    placed = (
        P("st", "tp"),
        P("st", "tp"),
        P("st", "tp"),
        P("st", None),
        P(),
        P(None, "tp"),
        P(None, "tp"),
        P("st", None),
        P("st", None),
    )
    return jax.shard_map(
        local,
        mesh=mesh,
        in_specs=placed,
        out_specs=(P("st", "tp"), P(("st", "tp"), None), P("st", "tp")),
        check_vma=False,
    )
```

```python
import functools

import jax
import jax.numpy as jnp
from jax import lax
from jax.experimental import pallas as pl
from jax.experimental.pallas import tpu as pltpu
from jax.sharding import PartitionSpec as P

HD = 128
PLEN = 64
EPS = 1e-06
NZ = 8
NJ = 8
NST = NZ * NJ
NTP = 4
MESH = pl.DeviceIdType.MESH
NT = (((1,), (1,)), ((), ()))
TN = (((0,), (0,)), ((), ()))
F32 = jnp.float32
BF16 = jnp.bfloat16


def dot(left, right, dims=(((1,), (0,)), ((), ()))):
    return lax.dot_general(left, right, dims, preferred_element_type=F32)


def row_scale(rows):
    return lax.rsqrt(jnp.mean(rows * rows, axis=-1, keepdims=True) + EPS)


def remote(src, dst, send_sem, recv_sem, axis, peer):
    return pltpu.make_async_remote_copy(
        src_ref=src, dst_ref=dst, send_sem=send_sem, recv_sem=recv_sem, device_id={axis: peer}, device_id_type=MESH
    )


def wait_bytes(ref, sem):
    pltpu.make_async_copy(ref, ref, sem).wait()


def greet(me, tp):
    z, j = me // NJ, me % NJ
    barrier = pltpu.get_barrier_semaphore()
    for t in range(1, NJ):
        pl.semaphore_signal(barrier, inc=1, device_id={"st": z * NJ + (j + t) % NJ}, device_id_type=MESH)
    for t in range(1, NZ):
        pl.semaphore_signal(barrier, inc=1, device_id={"st": (z + t) % NZ * NJ + j}, device_id_type=MESH)
    if tp is not None:
        for t in range(1, NTP):
            pl.semaphore_signal(barrier, inc=1, device_id={"tp": (tp + t) % NTP}, device_id_type=MESH)
    return barrier, NJ + NZ - 2 + (0 if tp is None else NTP - 1)


NY = NJ // 2


PASSAGES = 20
PART = PASSAGES // 2
BASE = 24
PREV, LAST, PLACE, NAMED, META_ROWS = 64, 68, 72, 73, 80


class Column:
    def __init__(self, me, z_send, z_recv, y_send, y_recv):
        self.z, self.j, self.long = me // NJ, me % NJ, 1 - 2 * (me % 2)
        self.z_send, self.z_recv, self.y_send, self.y_recv = z_send, z_recv, y_send, y_recv

    def plane(self, steps):
        return (self.z + steps * self.long + NZ) % NZ

    def step(self, side, number, src, dst):
        peer = self.plane(1 - 2 * side) * NJ + self.j
        return remote(src, dst, self.z_send.at[side], self.z_recv.at[number], "st", peer)

    def beside(self, steps, core):
        return (self.j // 2 + steps + NY) % NY * 2 + core

    def spread(self, src, dst, plane, recv_sem):
        z, j, core = self.z, self.j, self.j % 2
        pltpu.make_async_copy(src.at[plane * NJ + j], dst.at[plane * NJ + j], recv_sem).start()
        for steps, to in ((2, 0), (2, 1), (1, 0), (-1, 0), (1, 1), (-1, 1), (0, 1 - core)):
            other = self.beside(steps, to)
            remote(src.at[plane * NJ + other], dst.at[plane * NJ + j], self.y_send, recv_sem, "st", z * NJ + other).start()


class Outward(Column):
    def __init__(self, me, meta, table, near, far, picked, passed, column, fin, *sems):
        super().__init__(me, *sems)
        self.meta, self.table, self.near, self.far = meta, table, near, far
        self.picked, self.passed, self.column, self.fin = picked, passed, column, fin

    def launch(self, part, side):
        at = pl.ds(part * PART, PART)
        return self.step(side, 2 * side + part, self.table.at[at], self.near.at[side, at])

    def relay(self, part):
        at = pl.ds(part * PART, PART)
        return self.step(0, 4 + part, self.near.at[0, at], self.far.at[at])

    def hop(self, name):
        column, picked, passed, at = self.column, self.picked, self.passed, self.block
        return {
            "s2": lambda: self.step(1, 6, picked.at[0], column.at[at(self.plane(1))]),
            "s3": lambda: self.step(1, 7, picked.at[1], passed.at[1]),
            "s3b": lambda: self.step(1, 8, passed.at[1], column.at[at(self.plane(2))]),
            "l3": lambda: self.step(0, 9, picked.at[2], column.at[at(self.plane(-2))]),
            "l4": lambda: self.step(0, 10, picked.at[3], passed.at[0]),
            "l4b": lambda: self.step(0, 11, passed.at[0], column.at[at(self.plane(-3))]),
        }[name]()

    def block(self, plane):
        return pl.ds(plane * NJ, NJ)

    def pick(self, table, owner_plane, reader_plane, out, first):
        meta, owner = self.meta, owner_plane * NJ + self.j

        @pl.loop(0, NJ)
        def _(t):
            out[first + t] = table[jnp.maximum(meta[reader_plane * NJ + t, owner], 0)]

    def deliver(self, plane):
        self.spread(self.column, self.fin, plane, self.y_recv.at[0])

    def start(self, part):
        for side in range(2):
            self.launch(part, side).start()

    def own(self):
        self.pick(self.table, self.z, self.z, self.column, self.z * NJ)
        self.deliver(self.z)

    def forward(self, part):
        self.launch(part, 0).wait_recv()
        self.relay(part).start()

    def first(self):
        for part in range(2):
            self.launch(part, 1).wait_recv()
        owner = self.plane(1)
        self.pick(self.near.at[1], owner, self.plane(-2), self.picked.at[1], 0)
        self.hop("s3").start()
        self.pick(self.near.at[1], owner, self.plane(-1), self.picked.at[0], 0)
        self.hop("s2").start()
        for owner, side in ((self.plane(-1), 0), (self.plane(1), 1)):
            self.pick(self.near.at[side], owner, self.z, self.column, owner * NJ)
            self.deliver(owner)

    def second(self):
        self.hop("s3").wait_recv()
        self.hop("s3b").start()
        for part in range(2):
            self.relay(part).wait_recv()
        owner = self.plane(-2)
        self.pick(self.far, owner, self.plane(2), self.picked.at[3], 0)
        self.hop("l4").start()
        self.pick(self.far, owner, self.plane(1), self.picked.at[2], 0)
        self.hop("l3").start()
        self.pick(self.far, owner, self.z, self.column, owner * NJ)
        self.deliver(owner)
        self.hop("s2").wait_recv()
        self.deliver(self.plane(2))

    def third(self):
        self.hop("l4").wait_recv()
        self.hop("l4b").start()
        self.hop("s3b").wait_recv()
        self.deliver(self.plane(3))
        self.hop("l3").wait_recv()
        self.deliver(self.plane(-3))

    def fourth(self):
        self.hop("l4b").wait_recv()
        self.deliver(self.plane(-4))

    def arrive(self):
        wait_bytes(self.fin, self.y_recv.at[0])

    def finish(self):
        wait_bytes(self.column, self.z_send.at[0])
        wait_bytes(self.column.at[pl.ds(0, 44)], self.z_send.at[1])
        wait_bytes(self.column.at[pl.ds(0, NZ * (NJ - 1))], self.y_send)


class Homeward(Column):
    def __init__(self, me, meta, x, column, slots, sums, gained, stage, *sems):
        super().__init__(me, *sems)
        self.meta, self.x, self.column, self.slots = meta, x, column, slots
        self.sums, self.gained, self.stage = sums, gained, stage

    def block(self, plane):
        return pl.ds(plane * NJ, NJ)

    def hop(self, name):
        mine = lambda steps: self.column.at[self.block(self.plane(steps))]
        slots, sums, gained = self.slots, self.sums, self.gained
        return {
            "l4": lambda: self.step(1, 0, mine(-4), slots.at[0]),
            "l3": lambda: self.step(1, 1, mine(-3), slots.at[1]),
            "l4b": lambda: self.step(1, 2, slots.at[0], slots.at[2]),
            "s3": lambda: self.step(0, 9, mine(3), slots.at[3]),
            "s2": lambda: self.step(0, 10, mine(2), slots.at[4]),
            "s3b": lambda: self.step(0, 11, slots.at[3], slots.at[5]),
        }[name]()

    def summed(self, number, part):
        at = pl.ds(part * PART, PART)
        side = 0 if number == 2 else 1
        return self.step(side, 3 + 2 * number + part, self.sums.at[number, at], self.gained.at[number, at])

    def start(self, *steps):
        for one in steps:
            plane = self.plane(one)
            self.spread(self.x, self.column, plane, self.y_recv.at[plane])

    def gathered(self, steps):
        plane = self.plane(steps)
        wait_bytes(self.column.at[self.block(plane)], self.y_recv.at[plane])

    def chain(self, combo, planes, slots):
        meta, stage = self.meta, self.stage
        for half in range(stage.shape[0]):
            cols = pl.ds(half * HD, HD)
            for rank, (plane, (ref, start)) in enumerate(zip(planes, slots)):

                @pl.loop(0, NJ)
                def _(t):
                    before = stage[half, meta[PREV + combo, plane * NJ + t]]
                    stage[half, rank * NJ + t] = ref[start + t, :, cols].astype(F32) + before

    def close(self, combo, part, bases, store):
        meta, stage = self.meta, self.stage
        for half in range(stage.shape[0]):
            cols = pl.ds(half * HD, HD)

            @pl.loop(part * PART, part * PART + PART)
            def _(p):
                total = stage[half, meta[LAST + combo, p]]
                for base in bases:
                    total = total + base[p, :, cols].astype(F32)
                store(p, cols, total.astype(BF16))

    def ship(self, combo, number, base=None):
        def store(p, cols, value):
            self.sums[number, p, :, cols] = value

        for part in range(2):
            if base is not None:
                self.summed(base, part).wait_recv()
            self.close(combo, part, () if base is None else (self.gained.at[base],), store)
            self.summed(number, part).start()

    def first(self):
        self.gathered(-4)
        self.hop("l4").start()
        self.gathered(3)
        self.hop("s3").start()
        self.gathered(-3)
        self.hop("l3").start()
        self.gathered(2)
        self.hop("s2").start()

    def second(self):
        self.hop("l4").wait_recv()
        self.hop("l4b").start()
        self.hop("s3").wait_recv()
        self.hop("s3b").start()

    def third(self):
        self.gathered(-2)
        self.hop("l3").wait_recv()
        self.hop("l4b").wait_recv()
        planes = (self.plane(2), self.plane(1), self.z)
        slots = ((self.slots.at[2], 0), (self.slots.at[1], 0), (self.column, self.plane(-2) * NJ))
        self.chain(0, planes, slots)
        self.ship(0, 0)

    def third_short(self):
        self.gathered(1)
        self.hop("s2").wait_recv()
        self.hop("s3b").wait_recv()
        planes = (self.plane(-2), self.plane(-1), self.z)
        slots = ((self.slots.at[5], 0), (self.slots.at[4], 0), (self.column, self.plane(1) * NJ))
        self.chain(2, planes, slots)
        self.ship(2, 2)

    def fourth(self):
        self.gathered(-1)
        self.chain(1, (self.z,), ((self.column, self.plane(-1) * NJ),))
        self.ship(1, 1, 0)

    def collect(self, store):
        self.gathered(0)
        self.chain(3, (self.z,), ((self.column, self.z * NJ),))
        for part in range(2):
            self.summed(2, part).wait_recv()
            self.summed(1, part).wait_recv()
            self.close(3, part, (self.gained.at[1], self.gained.at[2]), store)

    def finish(self):
        wait_bytes(self.column, self.z_send.at[1])
        wait_bytes(self.column.at[pl.ds(0, 44)], self.z_send.at[0])
        wait_bytes(self.column.at[pl.ds(0, NZ * (NJ - 1))], self.y_send)


def plans(asked, me, place, named, meta):
    z, j, long = me // NJ, me % NJ, 1 - 2 * (me % 2)
    everyone = asked[...].reshape(NST, 128)
    meta[0:NST] = everyone
    lanes = lax.broadcasted_iota(jnp.int32, (NST, 128), 1)
    reader = lax.broadcasted_iota(jnp.int32, (NST, 128), 0)
    combos = ((-2, 2, 3, -1), (-1, 0, 1, -1), (1, -2, 3, 1), (0, 0, 1, 1))
    for number, (owner, start, count, way) in enumerate(combos):
        owner = (z + owner * long + NZ) % NZ * NJ + j
        start = (z + start * long + NZ) % NZ

        def rank(index):
            return ((index // NJ - start) * (way * long) + 2 * NZ) % NZ * NJ + index % NJ

        mine, other = rank(reader), rank(lanes)
        column = jnp.max(jnp.where(lanes == owner, everyone, -1), axis=1, keepdims=True)
        across = jnp.max(jnp.where(lanes == reader, column, -1), axis=0, keepdims=True)
        inside = mine < count * NJ
        before = jnp.max(jnp.where(inside & (mine < other) & (column == across), mine, -1), axis=0, keepdims=True)
        last = jnp.max(jnp.where(inside & (column == lanes), mine, -1), axis=0, keepdims=True)
        meta[PREV + number : PREV + number + 1] = jnp.where(before < 0, BASE, before)
        meta[LAST + number : LAST + number + 1] = jnp.where(last < 0, BASE, last)
    meta[PLACE : PLACE + 1] = place
    meta[NAMED : NAMED + 1] = named
    meta[NAMED + 1 : META_ROWS] = jnp.zeros((META_ROWS - NAMED - 1, 128), jnp.int32)


def kernel(
    owners, slots, q_in, gate_in, cot_in, store_in, wk_in, wv_in, gain,
    dq_out, gs_out, gw_ref,
    rows, tables, asked, plan, meta, q, g, near_k, near_v, far_k, far_v, picked, passed, out_column, fin_k, fin_v, x, column, slot_v, sum_v, gain_v,
    xk, columnk, slot_k, sum_k, gain_k, weights, terms, stage, stage_k, pv, pk, wide_w, own, gwb, rs1, rsb, rs2, gs,
    oz_send, oz_recv, oy_send, oy_recv, hz_send, hz_recv, hy_send, hy_recv,
    row_sem, ask_sem, in_sem, tp_sem, w_sem, rs_sem, out_sem,
):
    me = lax.axis_index("st")
    tp = lax.axis_index("tp")
    z, j = me // NJ, me % NJ
    core = me % 2
    scale = HD ** (-0.5)
    heads = q.shape[1] // HD
    width = q.shape[1]
    blocks = weights.shape[0]
    quarter = gs.shape[0]
    barrier, peers = greet(me, tp)
    slim = pl.ds(pl.multiple_of(tp * HD, HD), HD)

    def out_sems(n):
        return oz_send.at[n], oz_recv.at[n], oy_send.at[n], oy_recv.at[n]

    def home_sems(n):
        return hz_send.at[n], hz_recv.at[n], hy_send.at[n], hy_recv.at[n]

    fins = (fin_k, fin_v)
    ek, ev = (
        Outward(me, meta, tables.at[n], (near_k, near_v)[n], (far_k, far_v)[n], picked.at[n], passed.at[n], out_column.at[n], fins[n], *out_sems(n))
        for n in range(2)
    )
    bv = Homeward(me, meta, x, column, slot_v, sum_v, gain_v, stage, *home_sems(0))
    bk = [
        Homeward(me, meta, xk.at[h], columnk.at[h], slot_k.at[h], sum_k.at[h], gain_k.at[h], stage_k.at[h], *home_sems(1 + h))
        for h in range(2)
    ]

    weight_loads = [
        pltpu.make_async_copy(ref.at[:, :, pl.ds(h * HD, HD)], wide_w.at[n, h, :, :, slim], in_sem.at[2 * n + h])
        for n, ref in enumerate((wk_in, wv_in))
        for h in range(2)
    ]
    first_loads = [
        pltpu.make_async_copy(ref, x.at[pl.ds(n * NST // 2, NST // 2)], in_sem.at[7 + n])
        for n, ref in enumerate((wk_in, wv_in))
    ]
    token_loads = [
        pltpu.make_async_copy(q_in, q, in_sem.at[4]),
        pltpu.make_async_copy(cot_in, g, in_sem.at[5]),
        pltpu.make_async_copy(gate_in, pv.at[pl.ds(0, gate_in.shape[0])], in_sem.at[6]),
    ]
    count = rows.shape[0] // 256

    def chunk(i):
        return pl.ds(i * 256, 256)

    def row_load(i):
        return pltpu.make_async_copy(store_in.at[chunk(i)], rows.at[chunk(i)], row_sem.at[i])

    row_load(0).start()
    for load in first_loads:
        load.start()
    for i in range(1, count):
        row_load(i).start()
    for load in weight_loads + token_loads:
        load.start()

    lane = lax.broadcasted_iota(jnp.int32, (1, 128), 1)
    request = jnp.full((1, 128), -1, jnp.int32)
    place = jnp.zeros((1, 128), jnp.int32)
    named = jnp.zeros((1, 128), jnp.int32)
    per_block = owners.shape[0]
    for b in range(blocks):
        for i in range(per_block):
            at = b * per_block + i
            owner, slot = owners[i, b], slots[i, b]
            request = jnp.where(lane == owner, slot, request)
            place = jnp.where(lane == owner, at, place)
            named = jnp.where(lane == at, owner, named)
    asked[z, j] = request
    for load in first_loads:
        load.wait()

    def project(i):
        at = chunk(i)
        row_load(i).wait()

        @pl.loop(0, 8)
        def _(t):
            tile = pl.ds(i * 256 + t * 32, 32)
            raw = rows[tile].astype(F32)
            rows[tile] = (raw * row_scale(raw) * gain[...]).astype(BF16)

        for n in range(2):
            weight = x[pl.ds(n * NST // 2, NST // 2)].reshape(rows.shape[1], width)
            tables[n, pl.ds(4 * i, 4)] = dot(rows[at], weight).astype(BF16).reshape(4, PLEN, width)

    project(0)
    project(1)
    project(2)
    pl.semaphore_wait(barrier, peers)
    for t in range(1, NZ):
        other = (z + t) % NZ
        remote(asked.at[z, j], asked.at[z, j], ask_sem.at[0], ask_sem.at[1], "st", other * NJ + j).start()
    ek.start(0)
    project(3)
    project(4)
    ek.start(1)
    wait_bytes(asked.at[pl.ds(0, NZ - 1), 0], ask_sem.at[1])
    for t in range(1, NJ):
        remote(asked.at[:, j], asked.at[:, j], ask_sem.at[2], ask_sem.at[3], "st", z * NJ + (j + t) % NJ).start()
    ek.forward(0)
    ek.forward(1)
    ev.start(0)

    part = wide_w.shape[2] // 2
    half_rows = pl.ds(core * part, part)

    def weight_move(n, away):
        ref = wide_w.at[n, :, half_rows, :, slim]
        return remote(ref, ref, w_sem.at[0, n, away], w_sem.at[1, n, away], "tp", (tp + away) % NTP)

    def weight_pass(n, away):
        ref = wide_w.at[n, :, half_rows, :, pl.ds(pl.multiple_of((tp + NTP - away) % NTP * HD, HD), HD)]
        return remote(ref, ref, w_sem.at[2, n, away], w_sem.at[3, n, away], "st", me + 1 - 2 * core)

    for load in weight_loads:
        load.wait()
    for n in range(2):
        for away in range(1, NTP):
            weight_move(n, away).start()
    wait_bytes(asked.at[pl.ds(0, NJ - 1)], ask_sem.at[3])
    plans(asked, me, place, named, plan)
    sent_plan = pltpu.make_async_copy(plan, meta, ask_sem.at[4])
    sent_plan.start()
    for load in token_loads:
        load.wait()

    @pl.loop(0, blocks)
    def _(b):
        at = pl.ds(b * 128, 128)
        g[at] = (jax.nn.sigmoid(pv[at].astype(F32)) * g[at].astype(F32)).astype(BF16)

    for ref in (stage.at[0], stage.at[1], stage_k.at[0, 0], stage_k.at[1, 0]):
        ref[BASE] = jnp.zeros(stage.shape[2:], F32)
    sent_plan.wait()
    ek.first()
    ek.own()
    ek.second()
    ev.start(1)
    ek.third()
    ev.forward(0)
    ev.forward(1)
    ev.first()
    ek.fourth()
    ev.own()
    ek.arrive()

    def joined(n, b, cols):
        return jnp.concatenate([fins[n][meta[NAMED, b * 4 + i], :, cols] for i in range(4)], axis=0)

    def weigh(b):
        at = pl.ds(b * 128, 128)
        for h in range(heads):
            cols = pl.ds(h * HD, HD)
            score = dot(joined(0, b, cols), q[at, cols], NT) * scale
            raised = jnp.exp(score - jnp.max(score, axis=0, keepdims=True))
            weight = raised / jnp.sum(raised, axis=0, keepdims=True)
            weight = weight.astype(BF16)
            weights[b, h] = weight
            terms[pl.ds(b * 4, 4), :, cols] = dot(weight, g[at, cols]).astype(BF16).reshape(4, PLEN, HD)

    pl.loop(0, blocks // 4)(weigh)
    ev.second()
    pl.loop(blocks // 4, blocks)(weigh)

    @pl.loop(0, NST)
    def _(o):
        x[o] = terms[meta[PLACE, o]]

    bv.start(-4, 3, -3, 2, -2)
    ev.third()
    ev.fourth()
    bv.first()
    bv.start(1, -1, 0)
    for n in range(2):
        for away in range(1, NTP):
            weight_move(n, away).wait_recv()
            weight_pass(n, away).start()
    bv.second()
    ev.arrive()
    bv.third()

    @pl.loop(0, blocks)
    def _(b):
        at = pl.ds(b * 128, 128)
        for h in range(heads):
            cols = pl.ds(h * HD, HD)
            steep = dot(joined(1, b, cols), g[at, cols], NT)
            weight = weights[b, h].astype(F32)
            delta = jnp.sum(weight * steep, axis=0, keepdims=True)
            slope = (weight * (steep - delta)).astype(BF16)
            terms[pl.ds(b * 4, 4), :, cols] = (dot(slope, q[at, cols]) * scale).astype(BF16).reshape(4, PLEN, HD)
            q[at, cols] = (dot(slope, joined(0, b, cols), TN) * scale).astype(BF16)

    dq_store = pltpu.make_async_copy(q, dq_out, out_sem.at[0])
    dq_store.start()

    @pl.loop(0, NST)
    def _(o):
        for h in range(2):
            xk[h, o] = terms[meta[PLACE, o], :, pl.ds(h * HD, HD)]

    bk[0].start(-4, 3, -3, 2, -2)
    bv.third_short()
    bk[0].first()
    bk[0].start(1, -1, 0)
    bk[1].start(-4, 3, -3, 2, -2)
    bv.fourth()
    bk[0].second()
    bk[1].first()
    bk[1].start(1, -1, 0)

    def keep(ref):
        def store(p, cols, value):
            ref[pl.ds(pl.multiple_of(p * PLEN, PLEN), PLEN), cols] = value

        return store

    bv.collect(keep(pv))

    def across(n, away):
        src = (pk.at[0], pk.at[1], pv.at[:, pl.ds(0, HD)], pv.at[:, pl.ds(HD, HD)])[n]
        peer = (tp + away) % NTP
        at = pl.ds(pl.multiple_of(peer * quarter, 16), quarter)
        return remote(src.at[at], own.at[n, :, slim], tp_sem.at[0, n, away], tp_sem.at[1, n, away], "tp", peer)

    def kept(n):
        src = (pk.at[0], pk.at[1], pv.at[:, pl.ds(0, HD)], pv.at[:, pl.ds(HD, HD)])[n]
        return pltpu.make_async_copy(src.at[pl.ds(pl.multiple_of(tp * quarter, 16), quarter)], own.at[n, :, slim], tp_sem.at[0, n, 0])

    def exchange(n):
        kept(n).start()
        for away in range(1, NTP):
            across(n, away).start()

    def exchanged(n):
        kept(n).wait()
        for away in range(1, NTP):
            across(n, away).wait()

    def weight_rows(n, h, i):
        return wide_w[n, h, 4 * i : 4 * i + 4].reshape(256, HD * NTP)

    exchange(2)
    exchange(3)
    bk[0].third()
    bk[0].third_short()
    bk[1].second()
    for i in range(NZ):
        gwb[i] = dot(rows[:, i * 256 : (i + 1) * 256], pv[...], TN).astype(BF16).reshape(NJ, 32, width)
    own_rows = pltpu.make_async_copy(
        store_in.at[pl.ds(pl.multiple_of(tp * quarter, 16), quarter)], rows.at[pl.ds(0, quarter)], out_sem.at[1]
    )
    own_rows.start()
    for t in range(1, NJ):
        other = (j + t) % NJ
        remote(gwb.at[:, other], rs1.at[j], rs_sem.at[0], rs_sem.at[1], "st", z * NJ + other).start()
    bk[0].fourth()
    bk[1].third()
    bk[1].third_short()
    wait_bytes(rs1.at[pl.ds(0, NJ - 1)], rs_sem.at[1])
    total = gwb[:, j].astype(F32)
    for t in range(1, NJ):
        total = total + rs1[(j + t) % NJ].astype(F32)
    rsb[...] = total.astype(BF16)
    gw_ref[...] = gwb[z, j].astype(F32)
    for t in range(1, NJ):
        gw_ref[...] += rs1[(j + t) % NJ, z].astype(F32)
    for t in range(1, NZ):
        other = (z + t) % NZ
        remote(rsb.at[other], rs2.at[z], rs_sem.at[2], rs_sem.at[3], "st", other * NJ + j).start()
    bk[0].collect(keep(pk.at[0]))
    exchange(0)
    bk[1].fourth()
    for n in range(2):
        for away in range(1, NTP):
            weight_pass(n, away).wait_recv()
    exchanged(2)
    exchanged(3)
    for i in range(8):
        out = pl.ds(i * 256, 256)
        gs[:, out] = dot(own[2], weight_rows(1, 0, i), NT) + dot(own[3], weight_rows(1, 1, i), NT)
    wait_bytes(rs2.at[pl.ds(0, NZ - 1)], rs_sem.at[3])
    for t in range(1, NZ):
        gw_ref[...] += rs2[(z + t) % NZ].astype(F32)
    exchanged(0)
    for i in range(8):
        out = pl.ds(i * 256, 256)
        gs[:, out] += dot(own[0], weight_rows(0, 0, i), NT)
    own_rows.wait()
    bk[1].collect(keep(pk.at[1]))
    exchange(1)
    exchanged(1)

    def stores(i):
        at = pl.ds(i * 64, 64)
        return pltpu.make_async_copy(rows.at[pl.ds(quarter + i * 64, 64)], gs_out.at[at], out_sem.at[2 + i])

    for i in range(8):
        out = pl.ds(i * 256, 256)
        gs[:, out] += dot(own[1], weight_rows(0, 1, i), NT)
    for i in range(quarter // 64):

        @pl.loop(0, 2)
        def _(t):
            at = pl.ds(i * 64 + t * 32, 32)
            raw = rows[at].astype(F32)
            inverse = row_scale(raw)
            unit = raw * inverse
            grad_unit = gs[at] * gain[...]
            slope = inverse * (grad_unit - unit * jnp.mean(grad_unit * unit, axis=-1, keepdims=True))
            rows[pl.ds(quarter + i * 64 + t * 32, 32)] = slope.astype(BF16)

        stores(i).start()

    for trip in (ek, ev, bv, *bk):
        trip.finish()
    for n in range(2):
        for away in range(1, NTP):
            weight_move(n, away).wait_send()
            weight_pass(n, away).wait_send()
    wait_bytes(asked.at[pl.ds(0, NZ - 1), 0], ask_sem.at[0])
    wait_bytes(asked.at[pl.ds(0, NJ - 1)], ask_sem.at[2])
    wait_bytes(rs1.at[pl.ds(0, NJ - 1)], rs_sem.at[0])
    wait_bytes(rs2.at[pl.ds(0, NZ - 1)], rs_sem.at[2])
    dq_store.wait()
    for i in range(quarter // 64):
        stores(i).wait()


def local(queries, gate_pre, cotangent, store, store_gain, w_key, w_value, owners, slots):
    tokens, width = queries.shape
    rows, features = store.shape
    heads = width // HD
    blocks = tokens // 128
    quarter = rows // NTP
    vmem = pl.BlockSpec(memory_space=pltpu.VMEM)
    smem = pl.BlockSpec(memory_space=pltpu.SMEM)
    far = pl.BlockSpec(memory_space=pltpu.HBM)
    piece = (PLEN, width)
    slim = (PLEN, HD)
    dma = pltpu.SemaphoreType.DMA
    grad_queries, grad_store, grad_w_value = pl.pallas_call(
        kernel,
        out_shape=(
            jax.ShapeDtypeStruct((tokens, width), BF16),
            jax.ShapeDtypeStruct((quarter, features), BF16),
            jax.ShapeDtypeStruct((features // NST, width), F32),
        ),
        in_specs=[smem, smem] + [far] * 6 + [vmem],
        out_specs=(far, far, vmem),
        scratch_shapes=[
            pltpu.VMEM((rows, features), BF16),
            pltpu.VMEM((2, PASSAGES) + piece, BF16),
            pltpu.VMEM((NZ, NJ, 1, 128), jnp.int32),
            pltpu.VMEM((META_ROWS, 128), jnp.int32),
            pltpu.SMEM((META_ROWS, 128), jnp.int32),
            pltpu.VMEM((tokens, width), BF16),
            pltpu.VMEM((tokens, width), BF16),
            pltpu.VMEM((2, PASSAGES) + piece, BF16),
            pltpu.VMEM((2, PASSAGES) + piece, BF16),
            pltpu.VMEM((PASSAGES,) + piece, BF16),
            pltpu.VMEM((PASSAGES,) + piece, BF16),
            pltpu.VMEM((2, 4, NJ) + piece, BF16),
            pltpu.VMEM((2, 2, NJ) + piece, BF16),
            pltpu.VMEM((2, NST) + piece, BF16),
            pltpu.VMEM((NST,) + piece, BF16),
            pltpu.VMEM((NST,) + piece, BF16),
            pltpu.VMEM((NST,) + piece, BF16),
            pltpu.VMEM((NST,) + piece, BF16),
            pltpu.VMEM((6, NJ) + piece, BF16),
            pltpu.VMEM((3, PASSAGES) + piece, BF16),
            pltpu.VMEM((3, PASSAGES) + piece, BF16),
            pltpu.VMEM((2, NST) + slim, BF16),
            pltpu.VMEM((2, NST) + slim, BF16),
            pltpu.VMEM((2, 6, NJ) + slim, BF16),
            pltpu.VMEM((2, 3, PASSAGES) + slim, BF16),
            pltpu.VMEM((2, 3, PASSAGES) + slim, BF16),
            pltpu.VMEM((blocks, heads, 256, 128), BF16),
            pltpu.VMEM((blocks * 4,) + piece, BF16),
            pltpu.VMEM((2, BASE + 1) + slim, F32),
            pltpu.VMEM((2, 1, BASE + 1) + slim, F32),
            pltpu.VMEM((rows, width), BF16),
            pltpu.VMEM((2, rows, HD), BF16),
            pltpu.VMEM((2, 2, NST // 2, PLEN, HD * NTP), BF16),
            pltpu.VMEM((4, quarter, HD * NTP), BF16),
            pltpu.VMEM((NZ, NJ, features // NST, width), BF16),
            pltpu.VMEM((NJ, NZ, features // NST, width), BF16),
            pltpu.VMEM((NZ, features // NST, width), BF16),
            pltpu.VMEM((NZ, features // NST, width), BF16),
            pltpu.VMEM((quarter, features), F32),
            dma((2, 2)),
            dma((2, 12)),
            dma((2,)),
            dma((2, 1)),
            dma((3, 2)),
            dma((3, 12)),
            dma((3,)),
            dma((3, NZ)),
            dma((rows // 256,)),
            dma((5,)),
            dma((9,)),
            dma((2, 4, NTP)),
            dma((4, 2, NTP)),
            dma((4,)),
            dma((2 + quarter // 64,)),
        ],
        cost_estimate=pl.CostEstimate(flops=10**10, bytes_accessed=10**7, transcendentals=0),
        compiler_params=pltpu.CompilerParams(collective_id=0, has_side_effects=True, vmem_limit_bytes=67043328),
        name="passages",
    )(owners.T, slots.T, queries, gate_pre, cotangent, store, *(w.reshape(-1, PLEN, width) for w in (w_key, w_value)), store_gain[None])
    return (grad_queries.astype(F32), grad_store.astype(F32), grad_w_value)


def solution(mesh):
    placed = (
        P("st", "tp"),
        P("st", "tp"),
        P("st", "tp"),
        P("st", None),
        P(),
        P(None, "tp"),
        P(None, "tp"),
        P("st", None),
        P("st", None),
    )
    return jax.shard_map(
        local,
        mesh=mesh,
        in_specs=placed,
        out_specs=(P("st", "tp"), P(("st", "tp"), None), P("st", "tp")),
        check_vma=False,
    )
```

```python
import functools

import jax
import jax.numpy as jnp
from jax import lax
from jax.experimental import pallas as pl
from jax.experimental.pallas import tpu as pltpu
from jax.sharding import PartitionSpec as P

HD = 128
PLEN = 64
EPS = 1e-06
NZ = 8
NJ = 8
NST = NZ * NJ
NTP = 4
MESH = pl.DeviceIdType.MESH
NT = (((1,), (1,)), ((), ()))
TN = (((0,), (0,)), ((), ()))
F32 = jnp.float32
BF16 = jnp.bfloat16


def dot(left, right, dims=(((1,), (0,)), ((), ()))):
    return lax.dot_general(left, right, dims, preferred_element_type=F32)


def row_scale(rows):
    return lax.rsqrt(jnp.mean(rows * rows, axis=-1, keepdims=True) + EPS)


def remote(src, dst, send_sem, recv_sem, axis, peer):
    return pltpu.make_async_remote_copy(
        src_ref=src, dst_ref=dst, send_sem=send_sem, recv_sem=recv_sem, device_id={axis: peer}, device_id_type=MESH
    )


def wait_bytes(ref, sem):
    pltpu.make_async_copy(ref, ref, sem).wait()


def greet(me, tp):
    z, j = me // NJ, me % NJ
    barrier = pltpu.get_barrier_semaphore()
    for t in range(1, NJ):
        pl.semaphore_signal(barrier, inc=1, device_id={"st": z * NJ + (j + t) % NJ}, device_id_type=MESH)
    for t in range(1, NZ):
        pl.semaphore_signal(barrier, inc=1, device_id={"st": (z + t) % NZ * NJ + j}, device_id_type=MESH)
    if tp is not None:
        for t in range(1, NTP):
            pl.semaphore_signal(barrier, inc=1, device_id={"tp": (tp + t) % NTP}, device_id_type=MESH)
    return barrier, NJ + NZ - 2 + (0 if tp is None else NTP - 1)


NY = NJ // 2


PASSAGES = 20
PART = PASSAGES // 2
BASE = 24
PREV, LAST, PLACE, NAMED, META_ROWS = 64, 68, 72, 73, 80


class Column:
    def __init__(self, me, z_send, z_recv, y_send, y_recv):
        self.z, self.j, self.long = me // NJ, me % NJ, 1 - 2 * (me % 2)
        self.z_send, self.z_recv, self.y_send, self.y_recv = z_send, z_recv, y_send, y_recv

    def plane(self, steps):
        return (self.z + steps * self.long + NZ) % NZ

    def step(self, side, number, src, dst):
        peer = self.plane(1 - 2 * side) * NJ + self.j
        return remote(src, dst, self.z_send.at[side], self.z_recv.at[number], "st", peer)

    def beside(self, steps, core):
        return (self.j // 2 + steps + NY) % NY * 2 + core

    def spread(self, src, dst, plane, recv_sem):
        z, j, core = self.z, self.j, self.j % 2
        pltpu.make_async_copy(src.at[plane * NJ + j], dst.at[plane * NJ + j], recv_sem).start()
        for steps, to in ((2, 0), (2, 1), (1, 0), (-1, 0), (1, 1), (-1, 1), (0, 1 - core)):
            other = self.beside(steps, to)
            remote(src.at[plane * NJ + other], dst.at[plane * NJ + j], self.y_send, recv_sem, "st", z * NJ + other).start()


class Outward(Column):
    def __init__(self, me, meta, table, near, far, picked, passed, column, fin, *sems):
        super().__init__(me, *sems)
        self.meta, self.table, self.near, self.far = meta, table, near, far
        self.picked, self.passed, self.column, self.fin = picked, passed, column, fin

    def launch(self, part, side):
        at = pl.ds(part * PART, PART)
        return self.step(side, 2 * side + part, self.table.at[at], self.near.at[side, at])

    def relay(self, part):
        at = pl.ds(part * PART, PART)
        return self.step(0, 4 + part, self.near.at[0, at], self.far.at[at])

    def hop(self, name):
        column, picked, passed, at = self.column, self.picked, self.passed, self.block
        return {
            "s2": lambda: self.step(1, 6, picked.at[0], column.at[at(self.plane(1))]),
            "s3": lambda: self.step(1, 7, picked.at[1], passed.at[1]),
            "s3b": lambda: self.step(1, 8, passed.at[1], column.at[at(self.plane(2))]),
            "l3": lambda: self.step(0, 9, picked.at[2], column.at[at(self.plane(-2))]),
            "l4": lambda: self.step(0, 10, picked.at[3], passed.at[0]),
            "l4b": lambda: self.step(0, 11, passed.at[0], column.at[at(self.plane(-3))]),
        }[name]()

    def block(self, plane):
        return pl.ds(plane * NJ, NJ)

    def pick(self, table, owner_plane, reader_plane, out, first):
        meta, owner = self.meta, owner_plane * NJ + self.j

        @pl.loop(0, NJ)
        def _(t):
            out[first + t] = table[jnp.maximum(meta[reader_plane * NJ + t, owner], 0)]

    def deliver(self, plane):
        self.spread(self.column, self.fin, plane, self.y_recv.at[0])

    def start(self, part):
        for side in range(2):
            self.launch(part, side).start()

    def own(self):
        self.pick(self.table, self.z, self.z, self.column, self.z * NJ)
        self.deliver(self.z)

    def forward(self, part):
        self.launch(part, 0).wait_recv()
        self.relay(part).start()

    def first(self):
        for part in range(2):
            self.launch(part, 1).wait_recv()
        owner = self.plane(1)
        self.pick(self.near.at[1], owner, self.plane(-2), self.picked.at[1], 0)
        self.hop("s3").start()
        self.pick(self.near.at[1], owner, self.plane(-1), self.picked.at[0], 0)
        self.hop("s2").start()
        for owner, side in ((self.plane(-1), 0), (self.plane(1), 1)):
            self.pick(self.near.at[side], owner, self.z, self.column, owner * NJ)
            self.deliver(owner)

    def second(self):
        self.hop("s3").wait_recv()
        self.hop("s3b").start()
        for part in range(2):
            self.relay(part).wait_recv()
        owner = self.plane(-2)
        self.pick(self.far, owner, self.plane(2), self.picked.at[3], 0)
        self.hop("l4").start()
        self.pick(self.far, owner, self.plane(1), self.picked.at[2], 0)
        self.hop("l3").start()
        self.pick(self.far, owner, self.z, self.column, owner * NJ)
        self.deliver(owner)
        self.hop("s2").wait_recv()
        self.deliver(self.plane(2))

    def third(self):
        self.hop("l4").wait_recv()
        self.hop("l4b").start()

    def third_rest(self):
        self.hop("s3b").wait_recv()
        self.deliver(self.plane(3))
        self.hop("l3").wait_recv()
        self.deliver(self.plane(-3))

    def fourth(self):
        self.hop("l4b").wait_recv()
        self.deliver(self.plane(-4))

    def arrive(self):
        wait_bytes(self.fin, self.y_recv.at[0])

    def finish(self):
        wait_bytes(self.column, self.z_send.at[0])
        wait_bytes(self.column.at[pl.ds(0, 44)], self.z_send.at[1])
        wait_bytes(self.column.at[pl.ds(0, NZ * (NJ - 1))], self.y_send)


class Homeward(Column):
    def __init__(self, me, meta, x, column, slots, sums, gained, stage, *sems):
        super().__init__(me, *sems)
        self.meta, self.x, self.column, self.slots = meta, x, column, slots
        self.sums, self.gained, self.stage = sums, gained, stage

    def block(self, plane):
        return pl.ds(plane * NJ, NJ)

    def hop(self, name):
        mine = lambda steps: self.column.at[self.block(self.plane(steps))]
        slots, sums, gained = self.slots, self.sums, self.gained
        return {
            "l4": lambda: self.step(1, 0, mine(-4), slots.at[0]),
            "l3": lambda: self.step(1, 1, mine(-3), slots.at[1]),
            "l4b": lambda: self.step(1, 2, slots.at[0], slots.at[2]),
            "s3": lambda: self.step(0, 9, mine(3), slots.at[3]),
            "s2": lambda: self.step(0, 10, mine(2), slots.at[4]),
            "s3b": lambda: self.step(0, 11, slots.at[3], slots.at[5]),
        }[name]()

    def summed(self, number, part):
        at = pl.ds(part * PART, PART)
        side = 0 if number == 2 else 1
        return self.step(side, 3 + 2 * number + part, self.sums.at[number, at], self.gained.at[number, at])

    def start(self, *steps):
        for one in steps:
            plane = self.plane(one)
            self.spread(self.x, self.column, plane, self.y_recv.at[plane])

    def gathered(self, steps):
        plane = self.plane(steps)
        wait_bytes(self.column.at[self.block(plane)], self.y_recv.at[plane])

    def chain(self, combo, planes, slots):
        meta, stage = self.meta, self.stage
        for half in range(stage.shape[0]):
            cols = pl.ds(half * HD, HD)
            for rank, (plane, (ref, start)) in enumerate(zip(planes, slots)):

                @pl.loop(0, NJ)
                def _(t):
                    before = stage[half, meta[PREV + combo, plane * NJ + t]]
                    stage[half, rank * NJ + t] = ref[start + t, :, cols].astype(F32) + before

    def close(self, combo, part, bases, store):
        meta, stage = self.meta, self.stage
        for half in range(stage.shape[0]):
            cols = pl.ds(half * HD, HD)

            @pl.loop(part * PART, part * PART + PART)
            def _(p):
                total = stage[half, meta[LAST + combo, p]]
                for base in bases:
                    total = total + base[p, :, cols].astype(F32)
                store(p, cols, total.astype(BF16))

    def ship(self, combo, number, base=None):
        def store(p, cols, value):
            self.sums[number, p, :, cols] = value

        for part in range(2):
            if base is not None:
                self.summed(base, part).wait_recv()
            self.close(combo, part, () if base is None else (self.gained.at[base],), store)
            self.summed(number, part).start()

    def first(self):
        self.gathered(-4)
        self.hop("l4").start()
        self.gathered(3)
        self.hop("s3").start()
        self.gathered(-3)
        self.hop("l3").start()
        self.gathered(2)
        self.hop("s2").start()

    def second(self):
        self.hop("l4").wait_recv()
        self.hop("l4b").start()
        self.hop("s3").wait_recv()
        self.hop("s3b").start()

    def third(self):
        self.gathered(-2)
        self.hop("l3").wait_recv()
        self.hop("l4b").wait_recv()
        planes = (self.plane(2), self.plane(1), self.z)
        slots = ((self.slots.at[2], 0), (self.slots.at[1], 0), (self.column, self.plane(-2) * NJ))
        self.chain(0, planes, slots)
        self.ship(0, 0)

    def third_short(self):
        self.gathered(1)
        self.hop("s2").wait_recv()
        self.hop("s3b").wait_recv()
        planes = (self.plane(-2), self.plane(-1), self.z)
        slots = ((self.slots.at[5], 0), (self.slots.at[4], 0), (self.column, self.plane(1) * NJ))
        self.chain(2, planes, slots)
        self.ship(2, 2)

    def fourth(self):
        self.gathered(-1)
        self.chain(1, (self.z,), ((self.column, self.plane(-1) * NJ),))
        self.ship(1, 1, 0)

    def collect(self, store):
        self.gathered(0)
        self.chain(3, (self.z,), ((self.column, self.z * NJ),))
        for part in range(2):
            self.summed(2, part).wait_recv()
            self.summed(1, part).wait_recv()
            self.close(3, part, (self.gained.at[1], self.gained.at[2]), store)

    def finish(self):
        wait_bytes(self.column, self.z_send.at[1])
        wait_bytes(self.column.at[pl.ds(0, 44)], self.z_send.at[0])
        wait_bytes(self.column.at[pl.ds(0, NZ * (NJ - 1))], self.y_send)


def plans(asked, me, place, named, meta):
    z, j, long = me // NJ, me % NJ, 1 - 2 * (me % 2)
    everyone = asked[...].reshape(NST, 128)
    meta[0:NST] = everyone
    lanes = lax.broadcasted_iota(jnp.int32, (NST, 128), 1)
    reader = lax.broadcasted_iota(jnp.int32, (NST, 128), 0)
    combos = ((-2, 2, 3, -1), (-1, 0, 1, -1), (1, -2, 3, 1), (0, 0, 1, 1))
    for number, (owner, start, count, way) in enumerate(combos):
        owner = (z + owner * long + NZ) % NZ * NJ + j
        start = (z + start * long + NZ) % NZ

        def rank(index):
            return ((index // NJ - start) * (way * long) + 2 * NZ) % NZ * NJ + index % NJ

        mine, other = rank(reader), rank(lanes)
        column = jnp.max(jnp.where(lanes == owner, everyone, -1), axis=1, keepdims=True)
        across = jnp.max(jnp.where(lanes == reader, column, -1), axis=0, keepdims=True)
        inside = mine < count * NJ
        before = jnp.max(jnp.where(inside & (mine < other) & (column == across), mine, -1), axis=0, keepdims=True)
        last = jnp.max(jnp.where(inside & (column == lanes), mine, -1), axis=0, keepdims=True)
        meta[PREV + number : PREV + number + 1] = jnp.where(before < 0, BASE, before)
        meta[LAST + number : LAST + number + 1] = jnp.where(last < 0, BASE, last)
    meta[PLACE : PLACE + 1] = place
    meta[NAMED : NAMED + 1] = named
    meta[NAMED + 1 : META_ROWS] = jnp.zeros((META_ROWS - NAMED - 1, 128), jnp.int32)


def kernel(
    owners, slots, q_in, gate_in, cot_in, store_in, wk_in, wv_in, gain,
    dq_out, gs_out, gw_ref,
    rows, tables, asked, plan, meta, q, g, near_k, near_v, far_k, far_v, picked, passed, out_column, fin_k, fin_v, x, column, slot_v, sum_v, gain_v,
    xk, columnk, slot_k, sum_k, gain_k, weights, terms, stage, stage_k, pv, pk, wide_w, own, gwb, rs1, rsb, rs2, gs,
    oz_send, oz_recv, oy_send, oy_recv, hz_send, hz_recv, hy_send, hy_recv,
    row_sem, ask_sem, in_sem, tp_sem, w_sem, rs_sem, out_sem,
):
    me = lax.axis_index("st")
    tp = lax.axis_index("tp")
    z, j = me // NJ, me % NJ
    core = me % 2
    scale = HD ** (-0.5)
    heads = q.shape[1] // HD
    width = q.shape[1]
    blocks = weights.shape[0]
    quarter = gs.shape[0]
    barrier, peers = greet(me, tp)
    slim = pl.ds(pl.multiple_of(tp * HD, HD), HD)

    def out_sems(n):
        return oz_send.at[n], oz_recv.at[n], oy_send.at[n], oy_recv.at[n]

    def home_sems(n):
        return hz_send.at[n], hz_recv.at[n], hy_send.at[n], hy_recv.at[n]

    fins = (fin_k, fin_v)
    ek, ev = (
        Outward(me, meta, tables.at[n], (near_k, near_v)[n], (far_k, far_v)[n], picked.at[n], passed.at[n], out_column.at[n], fins[n], *out_sems(n))
        for n in range(2)
    )
    bv = Homeward(me, meta, x, column, slot_v, sum_v, gain_v, stage, *home_sems(0))
    bk = [
        Homeward(me, meta, xk.at[h], columnk.at[h], slot_k.at[h], sum_k.at[h], gain_k.at[h], stage_k.at[h], *home_sems(1 + h))
        for h in range(2)
    ]

    weight_loads = [
        pltpu.make_async_copy(ref.at[:, :, pl.ds(h * HD, HD)], wide_w.at[n, h, :, :, slim], in_sem.at[2 * n + h])
        for n, ref in enumerate((wk_in, wv_in))
        for h in range(2)
    ]
    first_loads = [
        pltpu.make_async_copy(ref, x.at[pl.ds(n * NST // 2, NST // 2)], in_sem.at[7 + n])
        for n, ref in enumerate((wk_in, wv_in))
    ]
    token_loads = [
        pltpu.make_async_copy(q_in, q, in_sem.at[4]),
        pltpu.make_async_copy(cot_in, g, in_sem.at[5]),
        pltpu.make_async_copy(gate_in, pv.at[pl.ds(0, gate_in.shape[0])], in_sem.at[6]),
    ]
    count = rows.shape[0] // 256

    def chunk(i):
        return pl.ds(i * 256, 256)

    def row_load(i):
        return pltpu.make_async_copy(store_in.at[chunk(i)], rows.at[chunk(i)], row_sem.at[i])

    row_load(0).start()
    for load in first_loads:
        load.start()
    for i in range(1, count):
        row_load(i).start()
    for load in weight_loads + token_loads:
        load.start()

    lane = lax.broadcasted_iota(jnp.int32, (1, 128), 1)
    request = jnp.full((1, 128), -1, jnp.int32)
    place = jnp.zeros((1, 128), jnp.int32)
    named = jnp.zeros((1, 128), jnp.int32)
    per_block = owners.shape[0]
    for b in range(blocks):
        for i in range(per_block):
            at = b * per_block + i
            owner, slot = owners[i, b], slots[i, b]
            request = jnp.where(lane == owner, slot, request)
            place = jnp.where(lane == owner, at, place)
            named = jnp.where(lane == at, owner, named)
    asked[z, j] = request
    for load in first_loads:
        load.wait()

    def project(i):
        at = chunk(i)
        row_load(i).wait()

        @pl.loop(0, 8)
        def _(t):
            tile = pl.ds(i * 256 + t * 32, 32)
            raw = rows[tile].astype(F32)
            rows[tile] = (raw * row_scale(raw) * gain[...]).astype(BF16)

        tabulate(0, i)

    def tabulate(n, i):
        weight = x[pl.ds(n * NST // 2, NST // 2)].reshape(rows.shape[1], width)
        tables[n, pl.ds(4 * i, 4)] = dot(rows[chunk(i)], weight).astype(BF16).reshape(4, PLEN, width)

    project(0)
    project(1)
    project(2)
    pl.semaphore_wait(barrier, peers)
    for t in range(1, NZ):
        other = (z + t) % NZ
        remote(asked.at[z, j], asked.at[z, j], ask_sem.at[0], ask_sem.at[1], "st", other * NJ + j).start()
    ek.start(0)
    project(3)
    project(4)
    ek.start(1)
    for i in range(count):
        tabulate(1, i)
    wait_bytes(asked.at[pl.ds(0, NZ - 1), 0], ask_sem.at[1])
    for t in range(1, NJ):
        remote(asked.at[:, j], asked.at[:, j], ask_sem.at[2], ask_sem.at[3], "st", z * NJ + (j + t) % NJ).start()
    ek.forward(0)
    ek.forward(1)
    ev.start(0)

    part = wide_w.shape[2] // 2
    half_rows = pl.ds(core * part, part)

    def weight_move(n, away):
        ref = wide_w.at[n, :, half_rows, :, slim]
        return remote(ref, ref, w_sem.at[0, n, away], w_sem.at[1, n, away], "tp", (tp + away) % NTP)

    def weight_pass(n, away):
        ref = wide_w.at[n, :, half_rows, :, pl.ds(pl.multiple_of((tp + NTP - away) % NTP * HD, HD), HD)]
        return remote(ref, ref, w_sem.at[2, n, away], w_sem.at[3, n, away], "st", me + 1 - 2 * core)

    for load in weight_loads:
        load.wait()
    for n in range(2):
        for away in range(1, NTP):
            weight_move(n, away).start()
    wait_bytes(asked.at[pl.ds(0, NJ - 1)], ask_sem.at[3])
    plans(asked, me, place, named, plan)
    sent_plan = pltpu.make_async_copy(plan, meta, ask_sem.at[4])
    sent_plan.start()
    for load in token_loads:
        load.wait()

    @pl.loop(0, blocks)
    def _(b):
        at = pl.ds(b * 128, 128)
        g[at] = (jax.nn.sigmoid(pv[at].astype(F32)) * g[at].astype(F32)).astype(BF16)

    for ref in (stage.at[0], stage.at[1], stage_k.at[0, 0], stage_k.at[1, 0]):
        ref[BASE] = jnp.zeros(stage.shape[2:], F32)
    sent_plan.wait()
    ek.first()
    ek.own()
    ev.own()
    ek.second()
    ek.third()
    ev.start(1)
    ek.third_rest()
    ev.forward(0)
    ev.forward(1)
    ev.first()
    ek.fourth()
    ek.arrive()

    def joined(n, b, cols):
        return jnp.concatenate([fins[n][meta[NAMED, b * 4 + i], :, cols] for i in range(4)], axis=0)

    def weigh(b):
        at = pl.ds(b * 128, 128)
        for h in range(heads):
            cols = pl.ds(h * HD, HD)
            score = dot(joined(0, b, cols), q[at, cols], NT) * scale
            raised = jnp.exp(score - jnp.max(score, axis=0, keepdims=True))
            weight = raised / jnp.sum(raised, axis=0, keepdims=True)
            weight = weight.astype(BF16)
            weights[b, h] = weight
            terms[pl.ds(b * 4, 4), :, cols] = dot(weight, g[at, cols]).astype(BF16).reshape(4, PLEN, HD)

    pl.loop(0, blocks // 4)(weigh)
    ev.second()
    pl.loop(blocks // 4, blocks)(weigh)

    @pl.loop(0, NST)
    def _(o):
        x[o] = terms[meta[PLACE, o]]

    bv.start(-4, 3, -3, 2, -2)
    ev.third()
    ev.third_rest()
    ev.fourth()
    bv.first()
    bv.start(1, -1, 0)
    for n in range(2):
        for away in range(1, NTP):
            weight_move(n, away).wait_recv()
            weight_pass(n, away).start()
    bv.second()
    ev.arrive()
    bv.third()

    @pl.loop(0, blocks)
    def _(b):
        at = pl.ds(b * 128, 128)
        for h in range(heads):
            cols = pl.ds(h * HD, HD)
            steep = dot(joined(1, b, cols), g[at, cols], NT)
            weight = weights[b, h].astype(F32)
            delta = jnp.sum(weight * steep, axis=0, keepdims=True)
            slope = (weight * (steep - delta)).astype(BF16)
            terms[pl.ds(b * 4, 4), :, cols] = (dot(slope, q[at, cols]) * scale).astype(BF16).reshape(4, PLEN, HD)
            q[at, cols] = (dot(slope, joined(0, b, cols), TN) * scale).astype(BF16)

    dq_store = pltpu.make_async_copy(q, dq_out, out_sem.at[0])
    dq_store.start()

    @pl.loop(0, NST)
    def _(o):
        for h in range(2):
            xk[h, o] = terms[meta[PLACE, o], :, pl.ds(h * HD, HD)]

    bk[0].start(-4, 3, -3, 2, -2)
    bv.third_short()
    bk[0].first()
    bk[0].start(1, -1, 0)
    bk[1].start(-4, 3, -3, 2, -2)
    bv.fourth()
    bk[0].second()
    bk[1].first()
    bk[1].start(1, -1, 0)

    def keep(ref):
        def store(p, cols, value):
            ref[pl.ds(pl.multiple_of(p * PLEN, PLEN), PLEN), cols] = value

        return store

    bv.collect(keep(pv))

    def across(n, away):
        src = (pk.at[0], pk.at[1], pv.at[:, pl.ds(0, HD)], pv.at[:, pl.ds(HD, HD)])[n]
        peer = (tp + away) % NTP
        at = pl.ds(pl.multiple_of(peer * quarter, 16), quarter)
        return remote(src.at[at], own.at[n, :, slim], tp_sem.at[0, n, away], tp_sem.at[1, n, away], "tp", peer)

    def kept(n):
        src = (pk.at[0], pk.at[1], pv.at[:, pl.ds(0, HD)], pv.at[:, pl.ds(HD, HD)])[n]
        return pltpu.make_async_copy(src.at[pl.ds(pl.multiple_of(tp * quarter, 16), quarter)], own.at[n, :, slim], tp_sem.at[0, n, 0])

    def exchange(n):
        kept(n).start()
        for away in range(1, NTP):
            across(n, away).start()

    def exchanged(n):
        kept(n).wait()
        for away in range(1, NTP):
            across(n, away).wait()

    def weight_rows(n, h, i):
        return wide_w[n, h, 4 * i : 4 * i + 4].reshape(256, HD * NTP)

    exchange(2)
    exchange(3)
    bk[0].third()
    bk[0].third_short()
    bk[1].second()
    for i in range(NZ):
        gwb[i] = dot(rows[:, i * 256 : (i + 1) * 256], pv[...], TN).astype(BF16).reshape(NJ, 32, width)
    own_rows = pltpu.make_async_copy(
        store_in.at[pl.ds(pl.multiple_of(tp * quarter, 16), quarter)], rows.at[pl.ds(0, quarter)], out_sem.at[1]
    )
    own_rows.start()
    for t in range(1, NJ):
        other = (j + t) % NJ
        remote(gwb.at[:, other], rs1.at[j], rs_sem.at[0], rs_sem.at[1], "st", z * NJ + other).start()
    bk[0].fourth()
    bk[1].third()
    bk[1].third_short()
    wait_bytes(rs1.at[pl.ds(0, NJ - 1)], rs_sem.at[1])
    total = gwb[:, j].astype(F32)
    for t in range(1, NJ):
        total = total + rs1[(j + t) % NJ].astype(F32)
    rsb[...] = total.astype(BF16)
    gw_ref[...] = gwb[z, j].astype(F32)
    for t in range(1, NJ):
        gw_ref[...] += rs1[(j + t) % NJ, z].astype(F32)
    for t in range(1, NZ):
        other = (z + t) % NZ
        remote(rsb.at[other], rs2.at[z], rs_sem.at[2], rs_sem.at[3], "st", other * NJ + j).start()
    bk[0].collect(keep(pk.at[0]))
    exchange(0)
    bk[1].fourth()
    for n in range(2):
        for away in range(1, NTP):
            weight_pass(n, away).wait_recv()
    exchanged(2)
    exchanged(3)
    for i in range(8):
        out = pl.ds(i * 256, 256)
        gs[:, out] = dot(own[2], weight_rows(1, 0, i), NT) + dot(own[3], weight_rows(1, 1, i), NT)
    wait_bytes(rs2.at[pl.ds(0, NZ - 1)], rs_sem.at[3])
    for t in range(1, NZ):
        gw_ref[...] += rs2[(z + t) % NZ].astype(F32)
    exchanged(0)
    for i in range(8):
        out = pl.ds(i * 256, 256)
        gs[:, out] += dot(own[0], weight_rows(0, 0, i), NT)
    own_rows.wait()
    bk[1].collect(keep(pk.at[1]))
    exchange(1)
    exchanged(1)

    def stores(i):
        at = pl.ds(i * 64, 64)
        return pltpu.make_async_copy(rows.at[pl.ds(quarter + i * 64, 64)], gs_out.at[at], out_sem.at[2 + i])

    for i in range(8):
        out = pl.ds(i * 256, 256)
        gs[:, out] += dot(own[1], weight_rows(0, 1, i), NT)
    for i in range(quarter // 64):

        @pl.loop(0, 2)
        def _(t):
            at = pl.ds(i * 64 + t * 32, 32)
            raw = rows[at].astype(F32)
            inverse = row_scale(raw)
            unit = raw * inverse
            grad_unit = gs[at] * gain[...]
            slope = inverse * (grad_unit - unit * jnp.mean(grad_unit * unit, axis=-1, keepdims=True))
            rows[pl.ds(quarter + i * 64 + t * 32, 32)] = slope.astype(BF16)

        stores(i).start()

    for trip in (ek, ev, bv, *bk):
        trip.finish()
    for n in range(2):
        for away in range(1, NTP):
            weight_move(n, away).wait_send()
            weight_pass(n, away).wait_send()
    wait_bytes(asked.at[pl.ds(0, NZ - 1), 0], ask_sem.at[0])
    wait_bytes(asked.at[pl.ds(0, NJ - 1)], ask_sem.at[2])
    wait_bytes(rs1.at[pl.ds(0, NJ - 1)], rs_sem.at[0])
    wait_bytes(rs2.at[pl.ds(0, NZ - 1)], rs_sem.at[2])
    dq_store.wait()
    for i in range(quarter // 64):
        stores(i).wait()


def local(queries, gate_pre, cotangent, store, store_gain, w_key, w_value, owners, slots):
    tokens, width = queries.shape
    rows, features = store.shape
    heads = width // HD
    blocks = tokens // 128
    quarter = rows // NTP
    vmem = pl.BlockSpec(memory_space=pltpu.VMEM)
    smem = pl.BlockSpec(memory_space=pltpu.SMEM)
    far = pl.BlockSpec(memory_space=pltpu.HBM)
    piece = (PLEN, width)
    slim = (PLEN, HD)
    dma = pltpu.SemaphoreType.DMA
    grad_queries, grad_store, grad_w_value = pl.pallas_call(
        kernel,
        out_shape=(
            jax.ShapeDtypeStruct((tokens, width), BF16),
            jax.ShapeDtypeStruct((quarter, features), BF16),
            jax.ShapeDtypeStruct((features // NST, width), F32),
        ),
        in_specs=[smem, smem] + [far] * 6 + [vmem],
        out_specs=(far, far, vmem),
        scratch_shapes=[
            pltpu.VMEM((rows, features), BF16),
            pltpu.VMEM((2, PASSAGES) + piece, BF16),
            pltpu.VMEM((NZ, NJ, 1, 128), jnp.int32),
            pltpu.VMEM((META_ROWS, 128), jnp.int32),
            pltpu.SMEM((META_ROWS, 128), jnp.int32),
            pltpu.VMEM((tokens, width), BF16),
            pltpu.VMEM((tokens, width), BF16),
            pltpu.VMEM((2, PASSAGES) + piece, BF16),
            pltpu.VMEM((2, PASSAGES) + piece, BF16),
            pltpu.VMEM((PASSAGES,) + piece, BF16),
            pltpu.VMEM((PASSAGES,) + piece, BF16),
            pltpu.VMEM((2, 4, NJ) + piece, BF16),
            pltpu.VMEM((2, 2, NJ) + piece, BF16),
            pltpu.VMEM((2, NST) + piece, BF16),
            pltpu.VMEM((NST,) + piece, BF16),
            pltpu.VMEM((NST,) + piece, BF16),
            pltpu.VMEM((NST,) + piece, BF16),
            pltpu.VMEM((NST,) + piece, BF16),
            pltpu.VMEM((6, NJ) + piece, BF16),
            pltpu.VMEM((3, PASSAGES) + piece, BF16),
            pltpu.VMEM((3, PASSAGES) + piece, BF16),
            pltpu.VMEM((2, NST) + slim, BF16),
            pltpu.VMEM((2, NST) + slim, BF16),
            pltpu.VMEM((2, 6, NJ) + slim, BF16),
            pltpu.VMEM((2, 3, PASSAGES) + slim, BF16),
            pltpu.VMEM((2, 3, PASSAGES) + slim, BF16),
            pltpu.VMEM((blocks, heads, 256, 128), BF16),
            pltpu.VMEM((blocks * 4,) + piece, BF16),
            pltpu.VMEM((2, BASE + 1) + slim, F32),
            pltpu.VMEM((2, 1, BASE + 1) + slim, F32),
            pltpu.VMEM((rows, width), BF16),
            pltpu.VMEM((2, rows, HD), BF16),
            pltpu.VMEM((2, 2, NST // 2, PLEN, HD * NTP), BF16),
            pltpu.VMEM((4, quarter, HD * NTP), BF16),
            pltpu.VMEM((NZ, NJ, features // NST, width), BF16),
            pltpu.VMEM((NJ, NZ, features // NST, width), BF16),
            pltpu.VMEM((NZ, features // NST, width), BF16),
            pltpu.VMEM((NZ, features // NST, width), BF16),
            pltpu.VMEM((quarter, features), F32),
            dma((2, 2)),
            dma((2, 12)),
            dma((2,)),
            dma((2, 1)),
            dma((3, 2)),
            dma((3, 12)),
            dma((3,)),
            dma((3, NZ)),
            dma((rows // 256,)),
            dma((5,)),
            dma((9,)),
            dma((2, 4, NTP)),
            dma((4, 2, NTP)),
            dma((4,)),
            dma((2 + quarter // 64,)),
        ],
        cost_estimate=pl.CostEstimate(flops=10**10, bytes_accessed=10**7, transcendentals=0),
        compiler_params=pltpu.CompilerParams(collective_id=0, has_side_effects=True, vmem_limit_bytes=67043328),
        name="passages",
    )(owners.T, slots.T, queries, gate_pre, cotangent, store, *(w.reshape(-1, PLEN, width) for w in (w_key, w_value)), store_gain[None])
    return (grad_queries.astype(F32), grad_store.astype(F32), grad_w_value)


def solution(mesh):
    placed = (
        P("st", "tp"),
        P("st", "tp"),
        P("st", "tp"),
        P("st", None),
        P(),
        P(None, "tp"),
        P(None, "tp"),
        P("st", None),
        P("st", None),
    )
    return jax.shard_map(
        local,
        mesh=mesh,
        in_specs=placed,
        out_specs=(P("st", "tp"), P(("st", "tp"), None), P("st", "tp")),
        check_vma=False,
    )
```

```python
import functools

import jax
import jax.numpy as jnp
from jax import lax
from jax.experimental import pallas as pl
from jax.experimental.pallas import tpu as pltpu
from jax.sharding import PartitionSpec as P

HD = 128
PLEN = 64
EPS = 1e-06
NZ = 8
NJ = 8
NST = NZ * NJ
NTP = 4
MESH = pl.DeviceIdType.MESH
NT = (((1,), (1,)), ((), ()))
TN = (((0,), (0,)), ((), ()))
F32 = jnp.float32
BF16 = jnp.bfloat16


def dot(left, right, dims=(((1,), (0,)), ((), ()))):
    return lax.dot_general(left, right, dims, preferred_element_type=F32)


def row_scale(rows):
    return lax.rsqrt(jnp.mean(rows * rows, axis=-1, keepdims=True) + EPS)


def remote(src, dst, send_sem, recv_sem, axis, peer):
    return pltpu.make_async_remote_copy(
        src_ref=src, dst_ref=dst, send_sem=send_sem, recv_sem=recv_sem, device_id={axis: peer}, device_id_type=MESH
    )


def wait_bytes(ref, sem):
    pltpu.make_async_copy(ref, ref, sem).wait()


def greet(me, tp):
    z, j = me // NJ, me % NJ
    barrier = pltpu.get_barrier_semaphore()
    for t in range(1, NJ):
        pl.semaphore_signal(barrier, inc=1, device_id={"st": z * NJ + (j + t) % NJ}, device_id_type=MESH)
    for t in range(1, NZ):
        pl.semaphore_signal(barrier, inc=1, device_id={"st": (z + t) % NZ * NJ + j}, device_id_type=MESH)
    if tp is not None:
        for t in range(1, NTP):
            pl.semaphore_signal(barrier, inc=1, device_id={"tp": (tp + t) % NTP}, device_id_type=MESH)
    return barrier, NJ + NZ - 2 + (0 if tp is None else NTP - 1)


NY = NJ // 2


PASSAGES = 20
PART = PASSAGES // 2
BASE = 24
PREV, LAST, PLACE, NAMED, META_ROWS = 64, 68, 72, 73, 80


class Column:
    def __init__(self, me, z_send, z_recv, y_send, y_recv):
        self.z, self.j, self.long = me // NJ, me % NJ, 1 - 2 * (me % 2)
        self.z_send, self.z_recv, self.y_send, self.y_recv = z_send, z_recv, y_send, y_recv

    def plane(self, steps):
        return (self.z + steps * self.long + NZ) % NZ

    def step(self, side, number, src, dst):
        peer = self.plane(1 - 2 * side) * NJ + self.j
        return remote(src, dst, self.z_send.at[side], self.z_recv.at[number], "st", peer)

    def beside(self, steps, core):
        return (self.j // 2 + steps + NY) % NY * 2 + core

    def spread(self, src, dst, plane, recv_sem):
        z, j, core = self.z, self.j, self.j % 2
        pltpu.make_async_copy(src.at[plane * NJ + j], dst.at[plane * NJ + j], recv_sem).start()
        for steps, to in ((2, 0), (2, 1), (1, 0), (-1, 0), (1, 1), (-1, 1), (0, 1 - core)):
            other = self.beside(steps, to)
            remote(src.at[plane * NJ + other], dst.at[plane * NJ + j], self.y_send, recv_sem, "st", z * NJ + other).start()


class Outward(Column):
    def __init__(self, me, meta, table, near, far, picked, passed, column, fin, *sems):
        super().__init__(me, *sems)
        self.meta, self.table, self.near, self.far = meta, table, near, far
        self.picked, self.passed, self.column, self.fin = picked, passed, column, fin

    def launch(self, part, side):
        at = pl.ds(part * PART, PART)
        return self.step(side, 2 * side + part, self.table.at[at], self.near.at[side, at])

    def relay(self, part):
        at = pl.ds(part * PART, PART)
        return self.step(0, 4 + part, self.near.at[0, at], self.far.at[at])

    def hop(self, name):
        column, picked, passed, at = self.column, self.picked, self.passed, self.block
        return {
            "s2": lambda: self.step(1, 6, picked.at[0], column.at[at(self.plane(1))]),
            "s3": lambda: self.step(1, 7, picked.at[1], passed.at[1]),
            "s3b": lambda: self.step(1, 8, passed.at[1], column.at[at(self.plane(2))]),
            "l3": lambda: self.step(0, 9, picked.at[2], column.at[at(self.plane(-2))]),
            "l4": lambda: self.step(0, 10, picked.at[3], passed.at[0]),
            "l4b": lambda: self.step(0, 11, passed.at[0], column.at[at(self.plane(-3))]),
        }[name]()

    def block(self, plane):
        return pl.ds(plane * NJ, NJ)

    def pick(self, table, owner_plane, reader_plane, out, first):
        meta, owner = self.meta, owner_plane * NJ + self.j

        @pl.loop(0, NJ)
        def _(t):
            out[first + t] = table[jnp.maximum(meta[reader_plane * NJ + t, owner], 0)]

    def deliver(self, plane):
        self.spread(self.column, self.fin, plane, self.y_recv.at[0])

    def start(self, part):
        for side in range(2):
            self.launch(part, side).start()

    def own(self):
        self.pick(self.table, self.z, self.z, self.column, self.z * NJ)
        self.deliver(self.z)

    def forward(self, part):
        self.launch(part, 0).wait_recv()
        self.relay(part).start()

    def first(self):
        for part in range(2):
            self.launch(part, 1).wait_recv()
        owner = self.plane(1)
        self.pick(self.near.at[1], owner, self.plane(-2), self.picked.at[1], 0)
        self.hop("s3").start()
        self.pick(self.near.at[1], owner, self.plane(-1), self.picked.at[0], 0)
        self.hop("s2").start()
        for owner, side in ((self.plane(-1), 0), (self.plane(1), 1)):
            self.pick(self.near.at[side], owner, self.z, self.column, owner * NJ)
            self.deliver(owner)

    def second(self):
        self.hop("s3").wait_recv()
        self.hop("s3b").start()
        for part in range(2):
            self.relay(part).wait_recv()
        owner = self.plane(-2)
        self.pick(self.far, owner, self.plane(2), self.picked.at[3], 0)
        self.hop("l4").start()
        self.pick(self.far, owner, self.plane(1), self.picked.at[2], 0)
        self.hop("l3").start()
        self.pick(self.far, owner, self.z, self.column, owner * NJ)
        self.deliver(owner)
        self.hop("s2").wait_recv()
        self.deliver(self.plane(2))

    def third(self):
        self.hop("l4").wait_recv()
        self.hop("l4b").start()

    def third_rest(self):
        self.hop("s3b").wait_recv()
        self.deliver(self.plane(3))
        self.hop("l3").wait_recv()
        self.deliver(self.plane(-3))

    def fourth(self):
        self.hop("l4b").wait_recv()
        self.deliver(self.plane(-4))

    def arrive(self):
        wait_bytes(self.fin, self.y_recv.at[0])

    def finish(self):
        wait_bytes(self.column, self.z_send.at[0])
        wait_bytes(self.column.at[pl.ds(0, 44)], self.z_send.at[1])
        wait_bytes(self.column.at[pl.ds(0, NZ * (NJ - 1))], self.y_send)


class Homeward(Column):
    def __init__(self, me, meta, x, column, slots, sums, gained, stage, *sems):
        super().__init__(me, *sems)
        self.meta, self.x, self.column, self.slots = meta, x, column, slots
        self.sums, self.gained, self.stage = sums, gained, stage

    def block(self, plane):
        return pl.ds(plane * NJ, NJ)

    def hop(self, name):
        mine = lambda steps: self.column.at[self.block(self.plane(steps))]
        slots, sums, gained = self.slots, self.sums, self.gained
        return {
            "l4": lambda: self.step(1, 0, mine(-4), slots.at[0]),
            "l3": lambda: self.step(1, 1, mine(-3), slots.at[1]),
            "l4b": lambda: self.step(1, 2, slots.at[0], slots.at[2]),
            "s3": lambda: self.step(0, 9, mine(3), slots.at[3]),
            "s2": lambda: self.step(0, 10, mine(2), slots.at[4]),
            "s3b": lambda: self.step(0, 11, slots.at[3], slots.at[5]),
        }[name]()

    def summed(self, number, part):
        at = pl.ds(part * PART, PART)
        side = 0 if number == 2 else 1
        return self.step(side, 3 + 2 * number + part, self.sums.at[number, at], self.gained.at[number, at])

    def start(self, *steps):
        for one in steps:
            plane = self.plane(one)
            self.spread(self.x, self.column, plane, self.y_recv.at[plane])

    def gathered(self, steps):
        plane = self.plane(steps)
        wait_bytes(self.column.at[self.block(plane)], self.y_recv.at[plane])

    def chain(self, combo, planes, slots):
        meta, stage = self.meta, self.stage
        for half in range(stage.shape[0]):
            cols = pl.ds(half * HD, HD)
            for rank, (plane, (ref, start)) in enumerate(zip(planes, slots)):

                @pl.loop(0, NJ)
                def _(t):
                    before = stage[half, meta[PREV + combo, plane * NJ + t]]
                    stage[half, rank * NJ + t] = ref[start + t, :, cols].astype(F32) + before

    def close(self, combo, part, bases, store):
        meta, stage = self.meta, self.stage
        for half in range(stage.shape[0]):
            cols = pl.ds(half * HD, HD)

            @pl.loop(part * PART, part * PART + PART)
            def _(p):
                total = stage[half, meta[LAST + combo, p]]
                for base in bases:
                    total = total + base[p, :, cols].astype(F32)
                store(p, cols, total.astype(BF16))

    def ship(self, combo, number, base=None):
        def store(p, cols, value):
            self.sums[number, p, :, cols] = value

        for part in range(2):
            if base is not None:
                self.summed(base, part).wait_recv()
            self.close(combo, part, () if base is None else (self.gained.at[base],), store)
            self.summed(number, part).start()

    def first(self):
        self.gathered(-4)
        self.hop("l4").start()
        self.gathered(3)
        self.hop("s3").start()
        self.gathered(-3)
        self.hop("l3").start()
        self.gathered(2)
        self.hop("s2").start()

    def second(self):
        self.hop("l4").wait_recv()
        self.hop("l4b").start()
        self.hop("s3").wait_recv()
        self.hop("s3b").start()

    def third(self):
        self.gathered(-2)
        self.hop("l3").wait_recv()
        self.hop("l4b").wait_recv()
        planes = (self.plane(2), self.plane(1), self.z)
        slots = ((self.slots.at[2], 0), (self.slots.at[1], 0), (self.column, self.plane(-2) * NJ))
        self.chain(0, planes, slots)
        self.ship(0, 0)

    def third_short(self):
        self.gathered(1)
        self.hop("s2").wait_recv()
        self.hop("s3b").wait_recv()
        planes = (self.plane(-2), self.plane(-1), self.z)
        slots = ((self.slots.at[5], 0), (self.slots.at[4], 0), (self.column, self.plane(1) * NJ))
        self.chain(2, planes, slots)
        self.ship(2, 2)

    def fourth(self):
        self.gathered(-1)
        self.chain(1, (self.z,), ((self.column, self.plane(-1) * NJ),))
        self.ship(1, 1, 0)

    def collect(self, store):
        self.gathered(0)
        self.chain(3, (self.z,), ((self.column, self.z * NJ),))
        for part in range(2):
            self.summed(2, part).wait_recv()
            self.summed(1, part).wait_recv()
            self.close(3, part, (self.gained.at[1], self.gained.at[2]), store)

    def finish(self):
        wait_bytes(self.column, self.z_send.at[1])
        wait_bytes(self.column.at[pl.ds(0, 44)], self.z_send.at[0])
        wait_bytes(self.column.at[pl.ds(0, NZ * (NJ - 1))], self.y_send)


def plans(asked, me, place, named, meta):
    z, j, long = me // NJ, me % NJ, 1 - 2 * (me % 2)
    everyone = asked[...].reshape(NST, 128)
    meta[0:NST] = everyone
    lanes = lax.broadcasted_iota(jnp.int32, (NST, 128), 1)
    reader = lax.broadcasted_iota(jnp.int32, (NST, 128), 0)
    combos = ((-2, 2, 3, -1), (-1, 0, 1, -1), (1, -2, 3, 1), (0, 0, 1, 1))
    for number, (owner, start, count, way) in enumerate(combos):
        owner = (z + owner * long + NZ) % NZ * NJ + j
        start = (z + start * long + NZ) % NZ

        def rank(index):
            return ((index // NJ - start) * (way * long) + 2 * NZ) % NZ * NJ + index % NJ

        mine, other = rank(reader), rank(lanes)
        column = jnp.max(jnp.where(lanes == owner, everyone, -1), axis=1, keepdims=True)
        across = jnp.max(jnp.where(lanes == reader, column, -1), axis=0, keepdims=True)
        inside = mine < count * NJ
        before = jnp.max(jnp.where(inside & (mine < other) & (column == across), mine, -1), axis=0, keepdims=True)
        last = jnp.max(jnp.where(inside & (column == lanes), mine, -1), axis=0, keepdims=True)
        meta[PREV + number : PREV + number + 1] = jnp.where(before < 0, BASE, before)
        meta[LAST + number : LAST + number + 1] = jnp.where(last < 0, BASE, last)
    meta[PLACE : PLACE + 1] = place
    meta[NAMED : NAMED + 1] = named
    meta[NAMED + 1 : META_ROWS] = jnp.zeros((META_ROWS - NAMED - 1, 128), jnp.int32)


def kernel(
    owners, slots, q_in, gate_in, cot_in, store_in, wk_in, wv_in, gain,
    dq_out, gs_out, gw_ref,
    rows, tables, asked, plan, meta, q, g, near_k, near_v, far_k, far_v, picked, passed, out_column, fin_k, fin_v, x, column, slot_v, sum_v, gain_v,
    xk, columnk, slot_k, sum_k, gain_k, weights, terms, stage, stage_k, pv, pk, wide_w, own, gwb, rs1, rsb, rs2, gs,
    oz_send, oz_recv, oy_send, oy_recv, hz_send, hz_recv, hy_send, hy_recv,
    row_sem, ask_sem, in_sem, tp_sem, w_sem, rs_sem, out_sem,
):
    me = lax.axis_index("st")
    tp = lax.axis_index("tp")
    z, j = me // NJ, me % NJ
    core = me % 2
    scale = HD ** (-0.5)
    heads = q.shape[1] // HD
    width = q.shape[1]
    blocks = weights.shape[0]
    quarter = gs.shape[0]
    barrier, peers = greet(me, tp)
    slim = pl.ds(pl.multiple_of(tp * HD, HD), HD)

    def out_sems(n):
        return oz_send.at[n], oz_recv.at[n], oy_send.at[n], oy_recv.at[n]

    def home_sems(n):
        return hz_send.at[n], hz_recv.at[n], hy_send.at[n], hy_recv.at[n]

    fins = (fin_k, fin_v)
    ek, ev = (
        Outward(me, meta, tables.at[n], (near_k, near_v)[n], (far_k, far_v)[n], picked.at[n], passed.at[n], out_column.at[n], fins[n], *out_sems(n))
        for n in range(2)
    )
    bv = Homeward(me, meta, x, column, slot_v, sum_v, gain_v, stage, *home_sems(0))
    bk = [
        Homeward(me, meta, xk.at[h], columnk.at[h], slot_k.at[h], sum_k.at[h], gain_k.at[h], stage_k.at[h], *home_sems(1 + h))
        for h in range(2)
    ]

    weight_loads = [
        pltpu.make_async_copy(ref.at[:, :, pl.ds(h * HD, HD)], wide_w.at[n, h, :, :, slim], in_sem.at[2 * n + h])
        for n, ref in enumerate((wk_in, wv_in))
        for h in range(2)
    ]
    first_loads = [
        pltpu.make_async_copy(ref, x.at[pl.ds(n * NST // 2, NST // 2)], in_sem.at[7 + n])
        for n, ref in enumerate((wk_in, wv_in))
    ]
    token_loads = [
        pltpu.make_async_copy(q_in, q, in_sem.at[4]),
        pltpu.make_async_copy(cot_in, g, in_sem.at[5]),
        pltpu.make_async_copy(gate_in, pv.at[pl.ds(0, gate_in.shape[0])], in_sem.at[6]),
    ]
    count = rows.shape[0] // 256

    def chunk(i):
        return pl.ds(i * 256, 256)

    def row_load(i):
        return pltpu.make_async_copy(store_in.at[chunk(i)], rows.at[chunk(i)], row_sem.at[i])

    row_load(0).start()
    for load in first_loads:
        load.start()
    for i in range(1, count):
        row_load(i).start()
    for load in weight_loads + token_loads:
        load.start()

    lane = lax.broadcasted_iota(jnp.int32, (1, 128), 1)
    request = jnp.full((1, 128), -1, jnp.int32)
    place = jnp.zeros((1, 128), jnp.int32)
    named = jnp.zeros((1, 128), jnp.int32)
    per_block = owners.shape[0]
    for b in range(blocks):
        for i in range(per_block):
            at = b * per_block + i
            owner, slot = owners[i, b], slots[i, b]
            request = jnp.where(lane == owner, slot, request)
            place = jnp.where(lane == owner, at, place)
            named = jnp.where(lane == at, owner, named)
    asked[z, j] = request
    for load in first_loads:
        load.wait()

    def project(i):
        at = chunk(i)
        row_load(i).wait()

        @pl.loop(0, 8)
        def _(t):
            tile = pl.ds(i * 256 + t * 32, 32)
            raw = rows[tile].astype(F32)
            rows[tile] = (raw * row_scale(raw) * gain[...]).astype(BF16)

        tabulate(0, i)

    def tabulate(n, i):
        weight = x[pl.ds(n * NST // 2, NST // 2)].reshape(rows.shape[1], width)
        tables[n, pl.ds(4 * i, 4)] = dot(rows[chunk(i)], weight).astype(BF16).reshape(4, PLEN, width)

    project(0)
    project(1)
    project(2)
    pl.semaphore_wait(barrier, peers)
    for t in range(1, NZ):
        other = (z + t) % NZ
        remote(asked.at[z, j], asked.at[z, j], ask_sem.at[0], ask_sem.at[1], "st", other * NJ + j).start()
    ek.start(0)
    project(3)
    project(4)
    ek.start(1)
    for i in range(count):
        tabulate(1, i)
    wait_bytes(asked.at[pl.ds(0, NZ - 1), 0], ask_sem.at[1])
    for t in range(1, NJ):
        remote(asked.at[:, j], asked.at[:, j], ask_sem.at[2], ask_sem.at[3], "st", z * NJ + (j + t) % NJ).start()
    ek.forward(0)
    ek.forward(1)
    ev.start(0)

    part = wide_w.shape[2] // 2
    half_rows = pl.ds(core * part, part)

    def weight_move(n, away):
        ref = wide_w.at[n, :, half_rows, :, slim]
        return remote(ref, ref, w_sem.at[0, n, away], w_sem.at[1, n, away], "tp", (tp + away) % NTP)

    def weight_pass(n, away):
        ref = wide_w.at[n, :, half_rows, :, pl.ds(pl.multiple_of((tp + NTP - away) % NTP * HD, HD), HD)]
        return remote(ref, ref, w_sem.at[2, n, away], w_sem.at[3, n, away], "st", me + 1 - 2 * core)

    for load in weight_loads:
        load.wait()
    for n in range(2):
        for away in range(1, NTP):
            weight_move(n, away).start()
    wait_bytes(asked.at[pl.ds(0, NJ - 1)], ask_sem.at[3])
    plans(asked, me, place, named, plan)
    sent_plan = pltpu.make_async_copy(plan, meta, ask_sem.at[4])
    sent_plan.start()
    for load in token_loads:
        load.wait()

    @pl.loop(0, blocks)
    def _(b):
        at = pl.ds(b * 128, 128)
        g[at] = (jax.nn.sigmoid(pv[at].astype(F32)) * g[at].astype(F32)).astype(BF16)

    for ref in (stage.at[0], stage.at[1], stage_k.at[0, 0], stage_k.at[1, 0]):
        ref[BASE] = jnp.zeros(stage.shape[2:], F32)
    sent_plan.wait()
    ek.first()
    ek.own()
    ev.own()
    ek.second()
    ek.third()
    ev.start(1)
    ek.third_rest()
    ev.forward(0)
    ev.forward(1)
    ev.first()
    ek.fourth()
    ek.arrive()

    def joined(n, b, cols):
        return jnp.concatenate([fins[n][meta[NAMED, b * 4 + i], :, cols] for i in range(4)], axis=0)

    def weigh(b):
        at = pl.ds(b * 128, 128)
        for h in range(heads):
            cols = pl.ds(h * HD, HD)
            score = dot(joined(0, b, cols), q[at, cols], NT) * scale
            raised = jnp.exp(score - jnp.max(score, axis=0, keepdims=True))
            weight = raised / jnp.sum(raised, axis=0, keepdims=True)
            weight = weight.astype(BF16)
            weights[b, h] = weight
            terms[pl.ds(b * 4, 4), :, cols] = dot(weight, g[at, cols]).astype(BF16).reshape(4, PLEN, HD)

    pl.loop(0, blocks // 4)(weigh)
    ev.second()
    pl.loop(blocks // 4, blocks)(weigh)

    @pl.loop(0, NST)
    def _(o):
        x[o] = terms[meta[PLACE, o]]

    bv.start(-4, 3, -3, 2, -2)
    ev.third()
    ev.third_rest()
    ev.fourth()
    bv.first()
    bv.start(1, -1, 0)
    for n in range(2):
        for away in range(1, NTP):
            weight_move(n, away).wait_recv()
            weight_pass(n, away).start()
    bv.second()
    ev.arrive()
    bv.third()

    @pl.loop(0, blocks)
    def _(b):
        at = pl.ds(b * 128, 128)
        for h in range(heads):
            cols = pl.ds(h * HD, HD)
            steep = dot(joined(1, b, cols), g[at, cols], NT)
            weight = weights[b, h].astype(F32)
            delta = jnp.sum(weight * steep, axis=0, keepdims=True)
            slope = (weight * (steep - delta)).astype(BF16)
            terms[pl.ds(b * 4, 4), :, cols] = (dot(slope, q[at, cols]) * scale).astype(BF16).reshape(4, PLEN, HD)
            q[at, cols] = (dot(slope, joined(0, b, cols), TN) * scale).astype(BF16)

    dq_store = pltpu.make_async_copy(q, dq_out, out_sem.at[0])
    dq_store.start()

    @pl.loop(0, NST)
    def _(o):
        for h in range(2):
            xk[h, o] = terms[meta[PLACE, o], :, pl.ds(h * HD, HD)]

    bk[0].start(-4, 3, -3, 2, -2)
    bv.third_short()
    bk[0].first()
    bv.fourth()
    bk[0].start(1, -1, 0)
    bk[1].start(-4, 3, -3, 2, -2)
    bk[0].second()
    bk[1].first()
    bk[1].start(1, -1, 0)

    def keep(ref):
        def store(p, cols, value):
            ref[pl.ds(pl.multiple_of(p * PLEN, PLEN), PLEN), cols] = value

        return store

    bv.collect(keep(pv))

    def across(n, away):
        src = (pk.at[0], pk.at[1], pv.at[:, pl.ds(0, HD)], pv.at[:, pl.ds(HD, HD)])[n]
        peer = (tp + away) % NTP
        at = pl.ds(pl.multiple_of(peer * quarter, 16), quarter)
        return remote(src.at[at], own.at[n, :, slim], tp_sem.at[0, n, away], tp_sem.at[1, n, away], "tp", peer)

    def kept(n):
        src = (pk.at[0], pk.at[1], pv.at[:, pl.ds(0, HD)], pv.at[:, pl.ds(HD, HD)])[n]
        return pltpu.make_async_copy(src.at[pl.ds(pl.multiple_of(tp * quarter, 16), quarter)], own.at[n, :, slim], tp_sem.at[0, n, 0])

    def exchange(n):
        kept(n).start()
        for away in range(1, NTP):
            across(n, away).start()

    def exchanged(n):
        kept(n).wait()
        for away in range(1, NTP):
            across(n, away).wait()

    def weight_rows(n, h, i):
        return wide_w[n, h, 4 * i : 4 * i + 4].reshape(256, HD * NTP)

    exchange(2)
    exchange(3)
    bk[0].third()
    bk[0].third_short()
    bk[1].second()
    for i in range(NZ):
        gwb[i] = dot(rows[:, i * 256 : (i + 1) * 256], pv[...], TN).astype(BF16).reshape(NJ, 32, width)
    own_rows = pltpu.make_async_copy(
        store_in.at[pl.ds(pl.multiple_of(tp * quarter, 16), quarter)], rows.at[pl.ds(0, quarter)], out_sem.at[1]
    )
    own_rows.start()
    for t in range(1, NJ):
        other = (j + t) % NJ
        remote(gwb.at[:, other], rs1.at[j], rs_sem.at[0], rs_sem.at[1], "st", z * NJ + other).start()
    bk[0].fourth()
    bk[1].third()
    bk[1].third_short()
    wait_bytes(rs1.at[pl.ds(0, NJ - 1)], rs_sem.at[1])
    total = gwb[:, j].astype(F32)
    for t in range(1, NJ):
        total = total + rs1[(j + t) % NJ].astype(F32)
    rsb[...] = total.astype(BF16)
    gw_ref[...] = gwb[z, j].astype(F32)
    for t in range(1, NJ):
        gw_ref[...] += rs1[(j + t) % NJ, z].astype(F32)
    for t in range(1, NZ):
        other = (z + t) % NZ
        remote(rsb.at[other], rs2.at[z], rs_sem.at[2], rs_sem.at[3], "st", other * NJ + j).start()
    bk[0].collect(keep(pk.at[0]))
    exchange(0)
    bk[1].fourth()
    for n in range(2):
        for away in range(1, NTP):
            weight_pass(n, away).wait_recv()
    exchanged(2)
    exchanged(3)
    for i in range(8):
        out = pl.ds(i * 256, 256)
        gs[:, out] = dot(own[2], weight_rows(1, 0, i), NT) + dot(own[3], weight_rows(1, 1, i), NT)
    wait_bytes(rs2.at[pl.ds(0, NZ - 1)], rs_sem.at[3])
    for t in range(1, NZ):
        gw_ref[...] += rs2[(z + t) % NZ].astype(F32)
    exchanged(0)
    for i in range(8):
        out = pl.ds(i * 256, 256)
        gs[:, out] += dot(own[0], weight_rows(0, 0, i), NT)
    own_rows.wait()
    bk[1].collect(keep(pk.at[1]))
    exchange(1)
    exchanged(1)

    def stores(i):
        at = pl.ds(i * 64, 64)
        return pltpu.make_async_copy(rows.at[pl.ds(quarter + i * 64, 64)], gs_out.at[at], out_sem.at[2 + i])

    for i in range(8):
        out = pl.ds(i * 256, 256)
        gs[:, out] += dot(own[1], weight_rows(0, 1, i), NT)
    for i in range(quarter // 64):

        @pl.loop(0, 2)
        def _(t):
            at = pl.ds(i * 64 + t * 32, 32)
            raw = rows[at].astype(F32)
            inverse = row_scale(raw)
            unit = raw * inverse
            grad_unit = gs[at] * gain[...]
            slope = inverse * (grad_unit - unit * jnp.mean(grad_unit * unit, axis=-1, keepdims=True))
            rows[pl.ds(quarter + i * 64 + t * 32, 32)] = slope.astype(BF16)

        stores(i).start()

    for trip in (ek, ev, bv, *bk):
        trip.finish()
    for n in range(2):
        for away in range(1, NTP):
            weight_move(n, away).wait_send()
            weight_pass(n, away).wait_send()
    wait_bytes(asked.at[pl.ds(0, NZ - 1), 0], ask_sem.at[0])
    wait_bytes(asked.at[pl.ds(0, NJ - 1)], ask_sem.at[2])
    wait_bytes(rs1.at[pl.ds(0, NJ - 1)], rs_sem.at[0])
    wait_bytes(rs2.at[pl.ds(0, NZ - 1)], rs_sem.at[2])
    dq_store.wait()
    for i in range(quarter // 64):
        stores(i).wait()


def local(queries, gate_pre, cotangent, store, store_gain, w_key, w_value, owners, slots):
    tokens, width = queries.shape
    rows, features = store.shape
    heads = width // HD
    blocks = tokens // 128
    quarter = rows // NTP
    vmem = pl.BlockSpec(memory_space=pltpu.VMEM)
    smem = pl.BlockSpec(memory_space=pltpu.SMEM)
    far = pl.BlockSpec(memory_space=pltpu.HBM)
    piece = (PLEN, width)
    slim = (PLEN, HD)
    dma = pltpu.SemaphoreType.DMA
    grad_queries, grad_store, grad_w_value = pl.pallas_call(
        kernel,
        out_shape=(
            jax.ShapeDtypeStruct((tokens, width), BF16),
            jax.ShapeDtypeStruct((quarter, features), BF16),
            jax.ShapeDtypeStruct((features // NST, width), F32),
        ),
        in_specs=[smem, smem] + [far] * 6 + [vmem],
        out_specs=(far, far, vmem),
        scratch_shapes=[
            pltpu.VMEM((rows, features), BF16),
            pltpu.VMEM((2, PASSAGES) + piece, BF16),
            pltpu.VMEM((NZ, NJ, 1, 128), jnp.int32),
            pltpu.VMEM((META_ROWS, 128), jnp.int32),
            pltpu.SMEM((META_ROWS, 128), jnp.int32),
            pltpu.VMEM((tokens, width), BF16),
            pltpu.VMEM((tokens, width), BF16),
            pltpu.VMEM((2, PASSAGES) + piece, BF16),
            pltpu.VMEM((2, PASSAGES) + piece, BF16),
            pltpu.VMEM((PASSAGES,) + piece, BF16),
            pltpu.VMEM((PASSAGES,) + piece, BF16),
            pltpu.VMEM((2, 4, NJ) + piece, BF16),
            pltpu.VMEM((2, 2, NJ) + piece, BF16),
            pltpu.VMEM((2, NST) + piece, BF16),
            pltpu.VMEM((NST,) + piece, BF16),
            pltpu.VMEM((NST,) + piece, BF16),
            pltpu.VMEM((NST,) + piece, BF16),
            pltpu.VMEM((NST,) + piece, BF16),
            pltpu.VMEM((6, NJ) + piece, BF16),
            pltpu.VMEM((3, PASSAGES) + piece, BF16),
            pltpu.VMEM((3, PASSAGES) + piece, BF16),
            pltpu.VMEM((2, NST) + slim, BF16),
            pltpu.VMEM((2, NST) + slim, BF16),
            pltpu.VMEM((2, 6, NJ) + slim, BF16),
            pltpu.VMEM((2, 3, PASSAGES) + slim, BF16),
            pltpu.VMEM((2, 3, PASSAGES) + slim, BF16),
            pltpu.VMEM((blocks, heads, 256, 128), BF16),
            pltpu.VMEM((blocks * 4,) + piece, BF16),
            pltpu.VMEM((2, BASE + 1) + slim, F32),
            pltpu.VMEM((2, 1, BASE + 1) + slim, F32),
            pltpu.VMEM((rows, width), BF16),
            pltpu.VMEM((2, rows, HD), BF16),
            pltpu.VMEM((2, 2, NST // 2, PLEN, HD * NTP), BF16),
            pltpu.VMEM((4, quarter, HD * NTP), BF16),
            pltpu.VMEM((NZ, NJ, features // NST, width), BF16),
            pltpu.VMEM((NJ, NZ, features // NST, width), BF16),
            pltpu.VMEM((NZ, features // NST, width), BF16),
            pltpu.VMEM((NZ, features // NST, width), BF16),
            pltpu.VMEM((quarter, features), F32),
            dma((2, 2)),
            dma((2, 12)),
            dma((2,)),
            dma((2, 1)),
            dma((3, 2)),
            dma((3, 12)),
            dma((3,)),
            dma((3, NZ)),
            dma((rows // 256,)),
            dma((5,)),
            dma((9,)),
            dma((2, 4, NTP)),
            dma((4, 2, NTP)),
            dma((4,)),
            dma((2 + quarter // 64,)),
        ],
        cost_estimate=pl.CostEstimate(flops=10**10, bytes_accessed=10**7, transcendentals=0),
        compiler_params=pltpu.CompilerParams(collective_id=0, has_side_effects=True, vmem_limit_bytes=67043328),
        name="passages",
    )(owners.T, slots.T, queries, gate_pre, cotangent, store, *(w.reshape(-1, PLEN, width) for w in (w_key, w_value)), store_gain[None])
    return (grad_queries.astype(F32), grad_store.astype(F32), grad_w_value)


def solution(mesh):
    placed = (
        P("st", "tp"),
        P("st", "tp"),
        P("st", "tp"),
        P("st", None),
        P(),
        P(None, "tp"),
        P(None, "tp"),
        P("st", None),
        P("st", None),
    )
    return jax.shard_map(
        local,
        mesh=mesh,
        in_specs=placed,
        out_specs=(P("st", "tp"), P(("st", "tp"), None), P("st", "tp")),
        check_vma=False,
    )
```
